256 devices in a mesh: ep: 64 (over z, y, core), tp: 4 (over x).
Axes of the slice: x: 4, y: 4, z: 8, core: 2. Of those that a mesh axis runs over, the one named last changes fastest.
Arguments:
- tokens: bfloat16 [1536, 1024], P('ep'), may hold values from -6 to 6
- mixer_gain: float32 [1024], replicated, may hold values from 0.1 to 1.9
- gate_weight: bfloat16 [1024, 1024], P(None, 'tp'), may hold values from -0.1875 to 0.1875
- inner_weight: bfloat16 [1024, 1024], P(None, 'tp'), may hold values from -0.1875 to 0.1875
- state_weight: bfloat16 [2, 1024, 512], P(None, None, 'tp'), may hold values from -0.1875 to 0.1875
- step_weight: bfloat16 [1024, 16], P(None, 'tp'), may hold values from -0.1875 to 0.1875
- step_bias: float32 [16], P('tp'), may hold values from -4 to 0.5
- decay_log: float32 [16], P('tp'), may hold values from 0 to 2.8
- skip_scale: float32 [16], P('tp'), may hold values from 0.5 to 1.5
- inner_kernel: float32 [4, 1024], P(None, 'tp'), may hold values from -3 to 3
- state_kernel: float32 [4, 2, 512], P(None, None, 'tp'), may hold values from -3 to 3
- inner_window: bfloat16 [1536, 3, 1024], P('ep', None, 'tp'), may hold values from -6 to 6
- state_window: bfloat16 [1536, 3, 2, 512], P('ep', None, None, 'tp'), may hold values from -6 to 6
- recurrent_state: float32 [1536, 16, 64, 128], P('ep', 'tp'), may hold values from -2.4 to 2.4
- group_gain: float32 [1024], P('tp'), may hold values from 0.1 to 1.9
- output_weight: bfloat16 [1024, 1024], P('tp'), may hold values from -0.1875 to 0.1875
- channel_gain: float32 [1024], replicated, may hold values from 0.1 to 1.9
- routes: int32 [1536, 2], P('ep'), may hold values from 0 to 63, all different within a row; in each aligned block of 24 rows (0 to 23, 24 to 47, ...) at most 2 rows name the same one
- route_weights: float32 [1536, 2], P('ep'), may hold values from 0.2 to 1
- expert_gate: bfloat16 [64, 1024, 2816], P('ep', None, 'tp'), may hold values from -0.1875 to 0.1875
- expert_up: bfloat16 [64, 1024, 2816], P('ep', None, 'tp'), may hold values from -0.1875 to 0.1875
- expert_down: bfloat16 [64, 2816, 1024], P('ep', 'tp'), may hold values from -0.109375 to 0.109375
- dense_gate: bfloat16 [1024, 2816], P('tp', 'ep'), may hold values from -0.1875 to 0.1875
- dense_up: bfloat16 [1024, 2816], P('tp', 'ep'), may hold values from -0.1875 to 0.1875
- dense_down: bfloat16 [2816, 1024], P('ep', 'tp'), may hold values from -0.109375 to 0.109375
- dense_scale: float32 [1024], P('tp'), may hold values from 0.3 to 1.5
Outputs:
- new_tokens: bfloat16 [1536, 1024], P('ep', 'tp')
- new_state: float32 [1536, 16, 64, 128], P('ep', 'tp')
- new_inner_window: bfloat16 [1536, 3, 1024], P('ep', None, 'tp')
- new_state_window: bfloat16 [1536, 3, 2, 512], P('ep', None, None, 'tp')
The draws below stay inside these ranges and needn't reach their ends.
Inputs may be any that keep to these rules, and one draw needn't show every extreme that they name: `routes`: each row names 2 different experts. Within the rows of one device (aligned blocks of 24 rows) no expert is named by more than 2 rows, and in some block an expert is named by exactly 2 rows.
All inputs are finite; a program needn't handle non-finite values.
Results may differ from the reference program's by a relative error of at most 0.014.
Values may be sent and summed in bfloat16 or wider, within the bound.
A program may use at most 64 MiB of HBM per device.

```python
import math
import jax
import jax.numpy as jnp
import numpy as np
from jax import lax

D = 1024
HEADS = 16
GROUPS = 4
HEAD_DIM = 64
STATE_DIM = 128
CONV = 4
FF = 2816
FFD = 2816
TOPK = 2
S_DEV = 24
EXPERTS = 64
BATCH = 1536
INNER = 1024
BC = 512
CAP = 2
N_EP = 64
N_TP = 4


def steps_of(own_key, dims, pieces, low, high):
    loudness, own = 1.0, jax.random.fold_in(own_key, 6)
    for axis_at, parts in pieces:
        draws = jnp.exp(jax.random.uniform(jax.random.fold_in(own, axis_at), (parts,), jnp.float32, low / len(pieces), high / len(pieces)))
        loudness = loudness * jnp.repeat(draws, dims[axis_at] // parts).reshape([-1 if axis == axis_at else 1 for axis in range(len(dims))])
    return loudness


def deal_out(own_key, own, number, rows, amount, top, bound, slope):
    order = jax.random.permutation(own_key, amount)
    crowded, ordinary = shares(amount, rows * top, bound, slope, True), shares(amount, rows * top, bound, slope, False)
    places = jnp.arange(amount)

    def named(sizes, offset_by):
        used = int((sizes > 0).sum())
        fixed = max(1, used // 4)
        shifted = fixed + (places - fixed + offset_by * (used - fixed)) % max(1, amount - fixed)
        return jnp.zeros((amount,), jnp.int32).at[order[jnp.where(places < fixed, places, shifted)]].set(jnp.asarray(sizes, jnp.int32))

    sizes = jnp.where(number % 4 == 0, named(crowded, number // 4), named(ordinary, number - number // 4 - 1))
    mixed = jax.random.permutation(jax.random.fold_in(own, 3), amount)
    giver, sink = mixed[0:amount // 2 * 2:2], mixed[1:amount // 2 * 2:2]
    room = jnp.minimum(sizes[giver] - 1, bound - sizes[sink]) // 2
    room = jnp.where((giver == order[0]) | (sink == order[0]) | (sizes[sink] == 0), 0, jnp.maximum(room, 0))
    shifted = jax.random.randint(jax.random.fold_in(own, 4), (amount // 2,), 0, 1 << 20) % (room + 1)
    sizes = sizes.at[giver].add(-shifted).at[sink].add(shifted)
    items = jnp.searchsorted(jnp.cumsum(sizes), jnp.arange(rows * top), side="right").astype(jnp.int32)
    listing = items.reshape(top, rows).T
    listing = listing[jax.random.permutation(jax.random.fold_in(own, 1), rows)]
    offset_by = jax.random.randint(jax.random.fold_in(own, 2), (rows, 1), 0, top)
    return jnp.take_along_axis(listing, (jnp.arange(top)[None, :] + offset_by) % top, axis=1)


def shares(count, total, bound, skew, full):
    weights = [(1 << 20) // math.isqrt(rank ** skew) + 1 for rank in range(1, count + 1)]
    largest = bound if full else min(bound, max(-(-total // count), total * weights[0] // sum(weights)))
    least = 1 if total - largest >= count - 1 else 0
    given, spare = [largest] + [least] * (count - 1), total - largest - least * (count - 1)
    while spare > 0:
        candidates = [i for i in range(1, count) if given[i] < largest] or [i for i in range(1, count) if given[i] < bound]
        pool, left = sum([weights[i] for i in candidates]), spare
        for i in candidates:
            addition = min(bound - given[i], max(1, left * weights[i] // pool), spare)
            given[i] = given[i] + addition
            spare = spare - addition
    return np.array(given)


def noise(own_key, extent, spread, most, shards=(), kind=jnp.bfloat16):
    array = jax.random.normal(own_key, extent, jnp.float32) * spread
    if len(shards) > 0:
        array = steps_of(own_key, extent, shards, -0.22, 0.18) * array
    return jnp.clip(array, min=-most, max=most).astype(kind)


def setup_inputs(seed: int = 0) -> dict:
    arg_keys = jax.random.split(jax.random.key(seed), 27)
    tokens = noise(arg_keys[0], (BATCH, D), 1.0, 6.0, ((0, 64),))
    mixer_gain = jnp.clip(1.0 + 0.18 * jax.random.normal(arg_keys[1], (D,), jnp.float32), 0.1, 1.9)
    gate_weight = noise(arg_keys[2], (D, INNER), D ** -0.5, 0.1875, ((1, 4),))
    inner_weight = noise(arg_keys[3], (D, INNER), D ** -0.5, 0.1875, ((1, 4),))
    state_weight = noise(arg_keys[4], (2, D, BC), D ** -0.5, 0.1875, ((2, 4),))
    step_weight = noise(arg_keys[5], (D, HEADS), D ** -0.5, 0.1875, ((1, 4),))
    step_bias = jnp.clip(-4.0 + 4.5 * jax.random.uniform(arg_keys[6], (HEADS,), jnp.float32) ** steps_of(arg_keys[6], (HEADS,), ((0, 4),), -0.2, 0.2), -4.0, 0.5)
    decay_log = jnp.clip(2.8 * jax.random.uniform(arg_keys[7], (HEADS,), jnp.float32) ** steps_of(arg_keys[7], (HEADS,), ((0, 4),), -0.2, 0.2), 0.0, 2.8)
    skip_scale = jnp.clip(0.5 + 1.0 * jax.random.uniform(arg_keys[8], (HEADS,), jnp.float32) ** steps_of(arg_keys[8], (HEADS,), ((0, 4),), -0.2, 0.2), 0.5, 1.5)
    inner_kernel = noise(arg_keys[9], (CONV, INNER), CONV ** -0.5, 3.0, ((1, 4),), jnp.float32)
    state_kernel = noise(arg_keys[10], (CONV, 2, BC), CONV ** -0.5, 3.0, ((2, 4),), jnp.float32)
    inner_window = noise(arg_keys[11], (BATCH, CONV - 1, INNER), 1.0, 6.0, ((0, 64), (2, 4)))
    state_window = noise(arg_keys[12], (BATCH, CONV - 1, 2, BC), 1.0, 6.0, ((0, 64), (3, 4)))
    recurrent_state = noise(arg_keys[13], (BATCH, HEADS, HEAD_DIM, STATE_DIM), 0.3, 2.4, ((0, 64), (1, 4)), jnp.float32)
    group_gain = jnp.clip(1.0 + 0.18 * jax.random.normal(arg_keys[14], (INNER,), jnp.float32), 0.1, 1.9)
    output_weight = noise(arg_keys[15], (INNER, D), INNER ** -0.5, 0.1875, ((0, 4),))
    channel_gain = jnp.clip(1.0 + 0.18 * jax.random.normal(arg_keys[16], (D,), jnp.float32), 0.1, 1.9)
    routes_keys = jax.random.split(jax.random.fold_in(arg_keys[17], 1), BATCH // S_DEV)
    routes_turns = jax.random.permutation(jax.random.fold_in(arg_keys[17], 3), BATCH // S_DEV)
    routes = jax.vmap(lambda own, number: deal_out(jax.random.fold_in(arg_keys[17], 2), own, number, S_DEV, EXPERTS, TOPK, CAP, 2))(routes_keys, routes_turns).reshape((BATCH, TOPK))
    route_weights = jnp.clip(0.2 + 0.8 * jax.random.uniform(arg_keys[18], (BATCH, TOPK), jnp.float32) ** steps_of(arg_keys[18], (BATCH, TOPK), ((0, 64),), -0.2, 0.2), 0.2, 1.0)
    expert_gate = noise(arg_keys[19], (EXPERTS, D, FF), D ** -0.5, 0.1875, ((0, 64), (2, 4)))
    expert_up = noise(arg_keys[20], (EXPERTS, D, FF), D ** -0.5, 0.1875, ((0, 64), (2, 4)))
    expert_down = noise(arg_keys[21], (EXPERTS, FF, D), FF ** -0.5, 0.109375, ((0, 64), (1, 4)))
    dense_gate = noise(arg_keys[22], (D, FFD), D ** -0.5, 0.1875, ((0, 4), (1, 64)))
    dense_up = noise(arg_keys[23], (D, FFD), D ** -0.5, 0.1875, ((0, 4), (1, 64)))
    dense_down = noise(arg_keys[24], (FFD, D), FFD ** -0.5, 0.109375, ((0, 64), (1, 4)))
    dense_scale = jnp.clip(0.3 + 1.2 * jax.random.uniform(arg_keys[25], (D,), jnp.float32) ** steps_of(arg_keys[25], (D,), ((0, 4),), -0.2, 0.2), 0.3, 1.5)
    return {"tokens": tokens, "mixer_gain": mixer_gain, "gate_weight": gate_weight, "inner_weight": inner_weight, "state_weight": state_weight, "step_weight": step_weight, "step_bias": step_bias, "decay_log": decay_log, "skip_scale": skip_scale, "inner_kernel": inner_kernel, "state_kernel": state_kernel, "inner_window": inner_window, "state_window": state_window, "recurrent_state": recurrent_state, "group_gain": group_gain, "output_weight": output_weight, "channel_gain": channel_gain, "routes": routes, "route_weights": route_weights, "expert_gate": expert_gate, "expert_up": expert_up, "expert_down": expert_down, "dense_gate": dense_gate, "dense_up": dense_up, "dense_down": dense_down, "dense_scale": dense_scale}


eps = 1e-06

def rms_scale(values, norm_gain):
    squares = lax.optimization_barrier(jnp.mean(values * values, axis=-1, keepdims=True))
    return values * lax.rsqrt(squares + eps) * norm_gain

def reference(tokens, mixer_gain, gate_weight, inner_weight, state_weight, step_weight, step_bias, decay_log, skip_scale, inner_kernel, state_kernel, inner_window, state_window, recurrent_state, group_gain, output_weight, channel_gain, routes, route_weights, expert_gate, expert_up, expert_down, dense_gate, dense_up, dense_down, dense_scale):
    f32 = jnp.float32
    bf16 = jnp.bfloat16
    residual = tokens.astype(f32)
    normed = rms_scale(residual, mixer_gain).astype(bf16)
    gate_pre = jnp.dot(normed, gate_weight, preferred_element_type=f32)
    inner_pre = jnp.dot(normed, inner_weight, preferred_element_type=f32).astype(bf16)
    state_pre = jnp.stack([jnp.dot(normed, state_weight[0], preferred_element_type=f32), jnp.dot(normed, state_weight[1], preferred_element_type=f32)], axis=1).astype(bf16)
    step_raw = jnp.dot(normed, step_weight, preferred_element_type=f32)
    inner_ctx = jnp.concatenate([inner_window, inner_pre[:, None, :]], axis=1)
    inner_conv = jax.nn.silu(lax.optimization_barrier(jnp.sum(inner_ctx.astype(f32) * inner_kernel[None], axis=1)))
    state_ctx = jnp.concatenate([state_window, state_pre[:, None]], axis=1)
    state_conv = jax.nn.silu(lax.optimization_barrier(jnp.sum(state_ctx.astype(f32) * state_kernel[None], axis=1)))
    per_group = HEADS // GROUPS
    step_size = jax.nn.softplus(step_raw + step_bias)
    decay_rate = jnp.exp(-step_size * jnp.exp(decay_log))
    shaped = (BATCH, GROUPS, per_group)
    inner_heads = inner_conv.reshape(BATCH, GROUPS, per_group, HEAD_DIM)
    in_vector = state_conv[:, 0].reshape(BATCH, GROUPS, STATE_DIM)
    out_vector = state_conv[:, 1].reshape(BATCH, GROUPS, STATE_DIM)
    old_state = recurrent_state.reshape(BATCH, GROUPS, per_group, HEAD_DIM, STATE_DIM)
    written = (step_size.reshape(shaped)[..., None] * inner_heads)[..., None] * in_vector[:, :, None, None, :]
    new_state = old_state * decay_rate.reshape(shaped)[..., None, None] + written
    mixed_out = jnp.einsum('sgrpn,sgn->sgrp', new_state, out_vector, precision=lax.Precision.HIGHEST)
    mixed_out = mixed_out + skip_scale.reshape(GROUPS, per_group)[None, :, :, None] * inner_heads
    gated_out = mixed_out.reshape(BATCH, INNER) * jax.nn.silu(gate_pre)
    grouped = rms_scale(gated_out.reshape(BATCH, GROUPS, -1), 1.0).reshape(BATCH, INNER)
    mixer_rows = (grouped * group_gain).astype(bf16)
    block_width = INNER // N_TP
    mixer_out = jnp.zeros((BATCH, D), f32)
    for block_index in range(N_TP):
        part_sum = jnp.dot(mixer_rows[:, block_index * block_width:(block_index + 1) * block_width], output_weight[block_index * block_width:(block_index + 1) * block_width], preferred_element_type=f32)
        mixer_out = mixer_out + lax.optimization_barrier(part_sum.astype(bf16)).astype(f32)
    residual = residual + mixer_out
    ffn_rows = rms_scale(residual, channel_gain).astype(bf16)
    dense_hidden = (jax.nn.silu(jnp.dot(ffn_rows, dense_gate, preferred_element_type=f32)) * jnp.dot(ffn_rows, dense_up, preferred_element_type=f32)).astype(bf16)
    dense_out = jnp.dot(dense_hidden, dense_down, preferred_element_type=f32)
    entries = S_DEV * TOPK
    flat_routes = routes.reshape(N_EP, entries)
    onehot = (flat_routes[:, :, None] == jnp.arange(EXPERTS, dtype=jnp.int32)[None, None, :]).astype(jnp.int32)
    rank_before = jnp.cumsum(onehot, axis=1) - onehot
    slot_index = lax.optimization_barrier(jnp.sum(rank_before * onehot, axis=2)).astype(jnp.int32)
    block_rows = ffn_rows.astype(f32).reshape(N_EP, S_DEV, D)
    hidden_width = FF // N_TP

    def one_expert(expert_id):
        chosen = (flat_routes == expert_id)[:, None, :] & (slot_index[:, None, :] == jnp.arange(CAP, dtype=jnp.int32)[None, :, None])
        chosen = lax.optimization_barrier(jnp.sum(chosen.astype(f32).reshape(N_EP, CAP, S_DEV, TOPK), axis=3))
        gathered = jnp.einsum('bcs,bsd->bcd', chosen, block_rows).astype(bf16).reshape(N_EP * CAP, D)
        gate_act = jnp.dot(gathered, expert_gate[expert_id], preferred_element_type=f32)
        up_act = jnp.dot(gathered, expert_up[expert_id], preferred_element_type=f32)
        activated = (jax.nn.silu(gate_act) * up_act).astype(bf16)
        down_whole = expert_down[expert_id]
        total = jnp.zeros((N_EP * CAP, D), f32)
        for block_index in range(N_TP):
            part_sum = jnp.dot(activated[:, block_index * hidden_width:(block_index + 1) * hidden_width], down_whole[block_index * hidden_width:(block_index + 1) * hidden_width], preferred_element_type=f32)
            total = total + lax.optimization_barrier(part_sum.astype(bf16)).astype(f32)
        return total.astype(bf16).reshape(N_EP, CAP, D)
    expert_rows = lax.map(one_expert, jnp.arange(EXPERTS, dtype=jnp.int32))
    block_ids = jnp.broadcast_to(jnp.arange(N_EP, dtype=jnp.int32)[:, None], (N_EP, entries))
    picked = expert_rows[flat_routes, block_ids, slot_index].astype(f32)
    weighted = picked.reshape(N_EP, S_DEV, TOPK, D) * route_weights.reshape(N_EP, S_DEV, TOPK)[..., None]
    expert_out = lax.optimization_barrier(jnp.sum(weighted, axis=2)).reshape(BATCH, D)
    new_tokens = (residual + expert_out + dense_scale * dense_out).astype(bf16)
    return (new_tokens, new_state.reshape(BATCH, HEADS, HEAD_DIM, STATE_DIM), inner_ctx[:, 1:], state_ctx[:, 1:])
```

```python
import functools

import jax
import jax.numpy as jnp
from jax import lax
from jax.experimental import pallas as pl
from jax.experimental.pallas import tpu as pltpu
from jax.sharding import PartitionSpec as P

MESH = pl.DeviceIdType.MESH
F32 = jnp.float32
BF16 = jnp.bfloat16
HEAD_DIM = 64
STATE_DIM = 128
NYC = 8
eps = 1e-06


def rms_scale(values, norm_gain):
    squares = jnp.mean(values * values, axis=-1, keepdims=True)
    return values * lax.rsqrt(squares + eps) * norm_gain


def dot(a, b):
    return jnp.dot(a, b, preferred_element_type=F32)


def mixer_kernel(
    tokens_ref,
    mixer_gain_ref,
    step_weight_ref,
    step_bias_ref,
    decay_log_ref,
    skip_ref,
    inner_kernel_ref,
    state_kernel_ref,
    inner_window_ref,
    state_window_ref,
    group_gain_ref,
    gate_weight_hbm,
    inner_weight_hbm,
    state_weight_hbm,
    output_weight_hbm,
    state_hbm,
    partial_ref,
    new_inner_ref,
    new_state_window_ref,
    new_state_hbm,
    gate_w,
    inner_w,
    state_w,
    output_w,
    state,
    in_sems,
    state_sems,
    out_sems,
):
    seqs = tokens_ref.shape[0]
    heads = state.shape[1]
    chunk = seqs // 4
    loads = [
        pltpu.make_async_copy(src, dst, in_sems.at[i])
        for i, (src, dst) in enumerate(
            [
                (inner_weight_hbm, inner_w),
                (state_weight_hbm, state_w),
                (gate_weight_hbm, gate_w),
                (output_weight_hbm, output_w),
            ]
        )
    ]
    for load in loads[:3]:
        load.start()
    state_loads = [
        pltpu.make_async_copy(
            state_hbm.at[pl.ds(c * chunk, chunk)], state.at[pl.ds(c * chunk, chunk)], state_sems.at[c]
        )
        for c in range(4)
    ]
    for load in state_loads:
        load.start()
    loads[3].start()

    residual = tokens_ref[...].astype(F32)
    normed = rms_scale(residual, mixer_gain_ref[...]).astype(BF16)
    step_raw = dot(normed, step_weight_ref[...])
    step_in = step_raw + step_bias_ref[...]
    step = jnp.maximum(step_in, 0.0) + jnp.log1p(jnp.exp(-jnp.abs(step_in)))
    decay = jnp.exp(-step * jnp.exp(decay_log_ref[...]))

    inner_window = inner_window_ref[...].astype(F32)
    loads[0].wait()
    inner_pre = dot(normed, inner_w[...]).astype(BF16).astype(F32)
    kern = inner_kernel_ref[...]
    conv = inner_pre * kern[3:4]
    for j in range(3):
        conv = conv + inner_window[:, j, :] * kern[j : j + 1]
    inner = jax.nn.silu(conv)
    new_inner_ref[...] = jnp.concatenate(
        [inner_window[:, 1:3, :], inner_pre[:, None, :]], axis=1
    ).astype(BF16)

    loads[1].wait()
    vectors = []
    pres = []
    for r in range(2):
        pre = dot(normed, state_w[r]).astype(BF16).astype(F32)
        conv = pre * state_kernel_ref[3, r : r + 1, :]
        for j in range(3):
            conv = conv + state_window_ref[:, j, r, :].astype(F32) * state_kernel_ref[j, r : r + 1, :]
        vectors.append(jax.nn.silu(conv))
        pres.append(pre)
    new_state_window_ref[:, 0:2] = state_window_ref[:, 1:3]
    new_state_window_ref[:, 2] = jnp.concatenate(
        [pres[0][:, None, :], pres[1][:, None, :]], axis=1
    ).astype(BF16)
    in_vector, out_vector = vectors

    loads[2].wait()
    gate_pre = dot(normed, gate_w[...])

    lane = lax.broadcasted_iota(jnp.int32, inner.shape, 1) // HEAD_DIM
    step_wide = jnp.broadcast_to(step[:, 0:1], inner.shape)
    skip_wide = jnp.broadcast_to(skip_ref[:, 0:1], inner.shape)
    for h in range(1, heads):
        step_wide = jnp.where(lane == h, step[:, h : h + 1], step_wide)
        skip_wide = jnp.where(lane == h, skip_ref[:, h : h + 1], skip_wide)
    written = jnp.transpose(step_wide * inner)

    columns = lax.broadcasted_iota(jnp.int32, (HEAD_DIM, STATE_DIM), 1)
    mixed = [jnp.zeros((HEAD_DIM, STATE_DIM), F32) for _ in range(heads)]
    stores = []
    for b in range(seqs):
        if b % chunk == 0:
            state_loads[b // chunk].wait()
        u = in_vector[b : b + 1, :]
        c = out_vector[b : b + 1, :]
        for h in range(heads):
            new = state[b, h] * decay[b : b + 1, h : h + 1] + (
                written[h * HEAD_DIM : (h + 1) * HEAD_DIM, b : b + 1] * u
            )
            state[b, h] = new
            read = jnp.sum(new * c, axis=1, keepdims=True)
            mixed[h] = jnp.where(columns == b, read, mixed[h])
        if b % chunk == chunk - 1:
            k = b // chunk
            store = pltpu.make_async_copy(
                state.at[pl.ds(k * chunk, chunk)], new_state_hbm.at[pl.ds(k * chunk, chunk)], out_sems.at[k]
            )
            store.start()
            stores.append(store)
    mixed_rows = jnp.transpose(jnp.concatenate(mixed, axis=0))[:seqs, :]
    mixed_rows = mixed_rows + skip_wide * inner
    gated = mixed_rows * jax.nn.silu(gate_pre)
    rows = (rms_scale(gated, 1.0) * group_gain_ref[...]).astype(BF16)
    loads[3].wait()
    partial_ref[...] = dot(rows, output_w[...]).astype(BF16)
    for store in stores:
        store.wait()


def ffn_kernel(
    n_ep,
    n_tp,
    partial_ref,
    tokens_ref,
    gain_ref,
    routes_ref,
    route_weights_ref,
    dense_gate_ref,
    dense_up_ref,
    dense_down_ref,
    dense_scale_ref,
    gate_hbm,
    up_hbm,
    down_hbm,
    out_ref,
    w_gate,
    w_up,
    w_down,
    parts,
    residual_ref,
    ffn_ref,
    gu,
    dn,
    dx,
    tall,
    going,
    came,
    xs,
    act,
    dz_going,
    dz_came,
    hid,
    moe_going,
    moe_came,
    tall_back,
    back_going,
    back_came,
    od_going,
    od_came,
    local_sems,
    send_sems,
    recv_sems,
):
    me = lax.axis_index("ep")
    t = lax.axis_index("tp")
    n_z = n_ep // NYC
    z = me // NYC
    yc = me % NYC
    seqs = tokens_ref.shape[0]
    width = out_ref.shape[1]
    slots = 2 * n_ep

    def across_tp(k):
        return (me, (t + k) % n_tp)

    def along_z(k):
        return (((z + k) % n_z) * NYC + yc, t)

    def within_z(k):
        return (z * NYC + (yc + k) % NYC, t)

    def along_ep(k):
        return ((me + k) % n_ep, t)

    def remote(src, dst, which, peer):
        return pltpu.make_async_remote_copy(
            src_ref=src,
            dst_ref=dst,
            send_sem=send_sems.at[which],
            recv_sem=recv_sems.at[which],
            device_id=peer,
            device_id_type=MESH,
        )

    def wait_in(ref, which):
        remote(ref, ref, which, across_tp(1)).wait_recv()

    def wait_out(ref, which):
        remote(ref, ref, which, across_tp(1)).wait_send()

    PART, GU, DN, DX, OUT, DZ, HID, MOE, BACK, OD = range(10)

    barrier = pltpu.get_barrier_semaphore()
    for k in range(1, n_tp):
        pl.semaphore_signal(barrier, inc=1, device_id=across_tp(k), device_id_type=MESH)

    def greet(k, carry):
        pl.semaphore_signal(barrier, inc=1, device_id=along_ep(k), device_id_type=MESH)
        return carry

    lax.fori_loop(1, n_ep, greet, 0)

    loads = [
        pltpu.make_async_copy(src.at[0], dst, local_sems.at[i])
        for i, (src, dst) in enumerate([(gate_hbm, w_gate), (up_hbm, w_up), (down_hbm, w_down)])
    ]
    for load in loads:
        load.start()

    units = dense_gate_ref.shape[1]
    gap = jnp.zeros((width, 64 - units), F32)
    gu[yc] = jnp.concatenate(
        [dense_gate_ref[...].astype(F32), gap, dense_up_ref[...].astype(F32), gap], axis=1
    ).astype(BF16)
    dn[yc] = jnp.concatenate(
        [dense_down_ref[...].astype(F32), jnp.zeros((64 - units, width), F32)], axis=0
    ).astype(BF16)
    parts[t] = partial_ref[...]

    expert = lax.broadcasted_iota(jnp.int32, (seqs, n_ep), 1)
    named = [(routes_ref[:, k : k + 1] == expert).astype(F32) for k in range(2)]
    earlier = (
        lax.broadcasted_iota(jnp.int32, (seqs, seqs), 0)
        > lax.broadcasted_iota(jnp.int32, (seqs, seqs), 1)
    ).astype(F32)
    before = dot(earlier, named[0] + named[1])
    place = lax.broadcasted_iota(jnp.int32, (seqs, slots), 1)
    chosen = []
    for k in range(2):
        slot = jnp.sum(before * named[k], axis=1, keepdims=True).astype(jnp.int32)
        chosen.append((place == routes_ref[:, k : k + 1] * 2 + slot).astype(F32))
    selection = jnp.transpose(chosen[0] + chosen[1]).astype(BF16)

    pl.semaphore_wait(barrier, n_tp - 1 + n_ep - 1)

    for k in range(1, n_tp):
        remote(partial_ref, parts.at[t], PART, across_tp(k)).start()

    def share_gate_up(k, carry):
        remote(gu.at[yc], gu.at[yc], GU, within_z(k)).start()
        return carry

    def share_down(k, carry):
        remote(dn.at[yc], dn.at[yc], DN, within_z(k)).start()
        return carry

    lax.fori_loop(1, NYC, share_gate_up, 0)
    lax.fori_loop(1, NYC, share_down, 0)

    wait_in(parts.at[pl.ds(0, n_tp - 1)], PART)
    total = parts[0].astype(F32)
    for k in range(1, n_tp):
        total = total + parts[k].astype(F32)
    residual = tokens_ref[...].astype(F32) + total
    residual_ref[...] = residual
    ffn = rms_scale(residual, gain_ref[...]).astype(BF16)
    ffn_ref[...] = ffn

    own = pl.ds(pl.multiple_of(t * width, width), width)
    dx[z] = ffn_ref[:, own]

    def share_tokens(k, carry):
        remote(dx.at[z], dx.at[z], DX, along_z(k)).start()
        return carry

    lax.fori_loop(1, n_z, share_tokens, 0)

    outgoing = dot(selection, ffn)
    lines = outgoing.shape[1] // 128
    for j in range(lines):
        tall[pl.ds(j, slots, stride=lines), :] = outgoing[:, j * 128 : (j + 1) * 128]
    going[...] = tall[...].reshape(going.shape).astype(BF16)

    def dispatch(k, carry):
        peer = along_ep(k)
        remote(going.at[peer[0]], came.at[me], OUT, peer).start()
        return carry

    lax.fori_loop(1, n_ep, dispatch, 0)
    came[me] = going[me]

    wait_in(gu.at[pl.ds(0, NYC - 1)], GU)
    wait_in(dx.at[pl.ds(0, n_z - 1)], DX)
    dense_rows = dx[...].reshape(n_z * seqs, width)
    for s in range(NYC):
        dz_going[:, :, s * 128 : (s + 1) * 128] = (
            dot(dense_rows, gu[s]).astype(BF16).reshape(n_tp, -1, 128)
        )
    for k in range(1, n_tp):
        peer = across_tp(k)
        remote(dz_going.at[peer[1]], dz_came.at[t], DZ, peer).start()
    dz_came[t] = dz_going[t]

    wait_in(came.at[pl.ds(0, n_ep - 1)], OUT)
    tall[...] = came[...].astype(F32).reshape(tall.shape)
    for j in range(lines):
        xs[:, j * 128 : (j + 1) * 128] = tall[pl.ds(j, slots, stride=lines), :].astype(BF16)
    loads[0].wait()
    loads[1].wait()
    rows = xs[...]
    act[...] = (jax.nn.silu(dot(rows, w_gate[...])) * dot(rows, w_up[...])).astype(BF16)
    loads[2].wait()
    for k in range(1, n_tp):
        peer = across_tp(k)
        columns = pl.ds(pl.multiple_of(peer[1] * width, width), width)
        moe_going[peer[1]] = dot(act[...], w_down[:, columns]).astype(BF16)
        remote(moe_going.at[peer[1]], moe_came.at[t], MOE, peer).start()
    moe_came[t] = dot(act[...], w_down[:, own]).astype(BF16)

    wait_in(dz_came.at[pl.ds(0, n_tp - 1)], DZ)
    low = lax.broadcasted_iota(jnp.int32, (dz_came.shape[1], 128), 1) < 64
    halves = []
    for s in range(NYC):
        block = dz_came[0, :, s * 128 : (s + 1) * 128].astype(F32)
        for k in range(1, n_tp):
            block = block + dz_came[k, :, s * 128 : (s + 1) * 128].astype(F32)
        up = pltpu.roll(block, 64, 1)
        halves.append(jax.nn.silu(block) * up)
    for s in range(NYC // 2):
        hid[t, :, s * 128 : (s + 1) * 128] = jnp.where(
            low, halves[2 * s], pltpu.roll(halves[2 * s + 1], 64, 1)
        ).astype(BF16)
    for k in range(1, n_tp):
        remote(hid.at[t], hid.at[t], HID, across_tp(k)).start()

    wait_in(moe_came.at[pl.ds(0, n_tp - 1)], MOE)
    rows_out = moe_came[0].astype(F32)
    for k in range(1, n_tp):
        rows_out = rows_out + moe_came[k].astype(F32)
    for j in range(width // 128):
        tall_back[pl.ds(j, slots, stride=4), :] = rows_out[:, j * 128 : (j + 1) * 128]
    back_going[...] = tall_back[...].reshape(back_going.shape).astype(BF16)

    def give_back(k, carry):
        peer = along_ep(k)
        remote(back_going.at[peer[0]], back_came.at[me], BACK, peer).start()
        return carry

    lax.fori_loop(1, n_ep, give_back, 0)
    back_came[me] = back_going[me]

    wait_in(dn.at[pl.ds(0, NYC - 1)], DN)
    wait_in(hid.at[pl.ds(0, n_tp - 1)], HID)
    dense_part = dot(
        hid[...].reshape(n_z * seqs, NYC * 64), dn[...].reshape(NYC * 64, width)
    )
    od_going[...] = dense_part.astype(BF16).reshape(od_going.shape)

    def share_out(k, carry):
        there = (z + k) % n_z
        remote(od_going.at[there], od_came.at[z], OD, along_z(k)).start()
        return carry

    lax.fori_loop(1, n_z, share_out, 0)
    od_came[z] = od_going[z]

    wait_in(od_came.at[pl.ds(0, n_z - 1)], OD)
    dense_out = od_came[0].astype(F32)
    for k in range(1, n_z):
        dense_out = dense_out + od_came[k].astype(F32)

    wait_in(back_came.at[pl.ds(0, n_ep - 1)], BACK)
    tall_back[...] = back_came[...].astype(F32).reshape(tall_back.shape)
    returned = [
        tall_back[pl.ds(j, slots, stride=4), :].astype(BF16) for j in range(width // 128)
    ]
    returned = jnp.concatenate(returned, axis=1)
    expert_out = jnp.zeros((seqs, width), F32)
    for k in range(2):
        expert_out = expert_out + route_weights_ref[:, k : k + 1] * dot(
            chosen[k].astype(BF16), returned
        )
    out_ref[...] = (
        residual_ref[:, own] + expert_out + dense_scale_ref[...] * dense_out
    ).astype(BF16)

    wait_out(parts.at[pl.ds(0, n_tp - 1)], PART)
    wait_out(gu.at[pl.ds(0, NYC - 1)], GU)
    wait_out(dn.at[pl.ds(0, NYC - 1)], DN)
    wait_out(dx.at[pl.ds(0, n_z - 1)], DX)
    wait_out(going.at[pl.ds(0, n_ep - 1)], OUT)
    wait_out(dz_going.at[pl.ds(0, n_tp - 1)], DZ)
    wait_out(hid.at[pl.ds(0, n_tp - 1)], HID)
    wait_out(moe_going.at[pl.ds(0, n_tp - 1)], MOE)
    wait_out(back_going.at[pl.ds(0, n_ep - 1)], BACK)
    wait_out(od_going.at[pl.ds(0, n_z - 1)], OD)


VMEM = pl.BlockSpec(memory_space=pltpu.VMEM)
ANY = pl.BlockSpec(memory_space=pl.ANY)


def local(
    n_ep,
    n_tp,
    tokens,
    mixer_gain,
    gate_weight,
    inner_weight,
    state_weight,
    step_weight,
    step_bias,
    decay_log,
    skip_scale,
    inner_kernel,
    state_kernel,
    inner_window,
    state_window,
    recurrent_state,
    group_gain,
    output_weight,
    channel_gain,
    routes,
    route_weights,
    expert_gate,
    expert_up,
    expert_down,
    dense_gate,
    dense_up,
    dense_down,
    dense_scale,
):
    seqs, model = tokens.shape
    width = dense_scale.shape[0]
    hidden = expert_gate.shape[2]
    n_z = n_ep // NYC
    slots = 2 * n_ep
    sds = jax.ShapeDtypeStruct
    partial, new_inner, new_window, new_state = pl.pallas_call(
        mixer_kernel,
        out_shape=(
            sds((seqs, model), BF16),
            sds(inner_window.shape, BF16),
            sds(state_window.shape, BF16),
            sds(recurrent_state.shape, F32),
        ),
        in_specs=[VMEM] * 11 + [ANY] * 5,
        out_specs=(VMEM, VMEM, VMEM, ANY),
        scratch_shapes=[
            pltpu.VMEM(gate_weight.shape, BF16),
            pltpu.VMEM(inner_weight.shape, BF16),
            pltpu.VMEM(state_weight.shape, BF16),
            pltpu.VMEM(output_weight.shape, BF16),
            pltpu.VMEM(recurrent_state.shape, F32),
            pltpu.SemaphoreType.DMA((4,)),
            pltpu.SemaphoreType.DMA((4,)),
            pltpu.SemaphoreType.DMA((4,)),
        ],
        name="mixer",
    )(
        tokens,
        mixer_gain[None],
        step_weight,
        step_bias[None],
        decay_log[None],
        skip_scale[None],
        inner_kernel,
        state_kernel,
        inner_window,
        state_window,
        group_gain[None],
        gate_weight,
        inner_weight,
        state_weight,
        output_weight,
        recurrent_state,
    )
    scratch = [
        pltpu.VMEM((model, hidden), BF16),
        pltpu.VMEM((model, hidden), BF16),
        pltpu.VMEM((hidden, model), BF16),
        pltpu.VMEM((n_tp, seqs, model), BF16),
        pltpu.VMEM((seqs, model), F32),
        pltpu.VMEM((seqs, model), BF16),
        pltpu.VMEM((NYC, width, 128), BF16),
        pltpu.VMEM((NYC, 64, width), BF16),
        pltpu.VMEM((n_z, seqs, width), BF16),
        pltpu.VMEM((slots * model // 128, 128), F32),
        pltpu.VMEM((n_ep, 2 * model // 128, 128), BF16),
        pltpu.VMEM((n_ep, 2 * model // 128, 128), BF16),
        pltpu.VMEM((slots, model), BF16),
        pltpu.VMEM((slots, hidden), BF16),
        pltpu.VMEM((n_tp, n_z * seqs // n_tp, NYC * 128), BF16),
        pltpu.VMEM((n_tp, n_z * seqs // n_tp, NYC * 128), BF16),
        pltpu.VMEM((n_tp, n_z * seqs // n_tp, NYC * 64), BF16),
        pltpu.VMEM((n_tp, slots, width), BF16),
        pltpu.VMEM((n_tp, slots, width), BF16),
        pltpu.VMEM((slots * 4, 128), F32),
        pltpu.VMEM((n_ep, 8, 128), BF16),
        pltpu.VMEM((n_ep, 8, 128), BF16),
        pltpu.VMEM((n_z, seqs, width), BF16),
        pltpu.VMEM((n_z, seqs, width), BF16),
        pltpu.SemaphoreType.DMA((3,)),
        pltpu.SemaphoreType.DMA((10,)),
        pltpu.SemaphoreType.DMA((10,)),
    ]
    new_tokens = pl.pallas_call(
        functools.partial(ffn_kernel, n_ep, n_tp),
        out_shape=sds((seqs, width), BF16),
        in_specs=[VMEM] * 9 + [ANY] * 3,
        out_specs=VMEM,
        scratch_shapes=scratch,
        compiler_params=pltpu.CompilerParams(collective_id=0, has_side_effects=True),
        name="ffn",
    )(
        partial,
        tokens,
        channel_gain[None],
        routes,
        route_weights,
        dense_gate,
        dense_up,
        dense_down,
        dense_scale[None],
        expert_gate,
        expert_up,
        expert_down,
    )
    return new_tokens, new_state, new_inner, new_window


def solution(mesh):
    placed = (
        P("ep", None),
        P(),
        P(None, "tp"),
        P(None, "tp"),
        P(None, None, "tp"),
        P(None, "tp"),
        P("tp"),
        P("tp"),
        P("tp"),
        P(None, "tp"),
        P(None, None, "tp"),
        P("ep", None, "tp"),
        P("ep", None, None, "tp"),
        P("ep", "tp", None, None),
        P("tp"),
        P("tp", None),
        P(),
        P("ep", None),
        P("ep", None),
        P("ep", None, "tp"),
        P("ep", None, "tp"),
        P("ep", "tp", None),
        P("tp", "ep"),
        P("tp", "ep"),
        P("ep", "tp"),
        P("tp"),
    )
    return jax.shard_map(
        functools.partial(local, mesh.shape["ep"], mesh.shape["tp"]),
        mesh=mesh,
        in_specs=placed,
        out_specs=(
            P("ep", "tp"),
            P("ep", "tp", None, None),
            P("ep", None, "tp"),
            P("ep", None, None, "tp"),
        ),
        check_vma=False,
    )
```

```python
import functools

import jax
import jax.numpy as jnp
from jax import lax
from jax.experimental import pallas as pl
from jax.experimental.pallas import tpu as pltpu
from jax.sharding import PartitionSpec as P

MESH = pl.DeviceIdType.MESH
F32 = jnp.float32
BF16 = jnp.bfloat16
HEAD_DIM = 64
STATE_DIM = 128
NYC = 8
UNITS = 48
eps = 1e-06


def rms_scale(values, norm_gain):
    squares = jnp.mean(values * values, axis=-1, keepdims=True)
    return values * lax.rsqrt(squares + eps) * norm_gain


def dot(a, b):
    return jnp.dot(a, b, preferred_element_type=F32)


def two_terms(v):
    high = v.astype(BF16).astype(F32)
    return high, (v - high).astype(BF16).astype(F32)


def dot_rows(a, b):
    return lax.dot_general(a, b, (((1,), (1,)), ((), ())), preferred_element_type=F32)


def mixer_kernel(
    tokens_ref,
    mixer_gain_ref,
    step_weight_ref,
    step_bias_ref,
    decay_log_ref,
    skip_ref,
    inner_kernel_ref,
    state_kernel_ref,
    inner_window_ref,
    state_window_ref,
    group_gain_ref,
    gate_weight_hbm,
    inner_weight_hbm,
    state_weight_hbm,
    output_weight_hbm,
    state_hbm,
    partial_ref,
    new_inner_ref,
    new_state_window_ref,
    new_state_hbm,
    gate_w,
    inner_w,
    state_w,
    output_w,
    state,
    decay_rows,
    read,
    in_sems,
    state_sems,
    out_sems,
):
    seqs = tokens_ref.shape[0]
    heads = state.shape[1]
    chunk = seqs // 4
    loads = [
        pltpu.make_async_copy(src, dst, in_sems.at[i])
        for i, (src, dst) in enumerate(
            [
                (inner_weight_hbm, inner_w),
                (state_weight_hbm, state_w),
                (gate_weight_hbm, gate_w),
                (output_weight_hbm, output_w),
            ]
        )
    ]
    for load in loads[:3]:
        load.start()
    state_loads = [
        pltpu.make_async_copy(
            state_hbm.at[pl.ds(c * chunk, chunk)], state.at[pl.ds(c * chunk, chunk)], state_sems.at[c]
        )
        for c in range(4)
    ]
    for load in state_loads:
        load.start()
    loads[3].start()

    residual = tokens_ref[...].astype(F32)
    normed = rms_scale(residual, mixer_gain_ref[...]).astype(BF16)
    step_raw = dot_rows(normed, step_weight_ref[...])
    step_in = step_raw + step_bias_ref[...]
    step = jnp.maximum(step_in, 0.0) + jnp.log1p(jnp.exp(-jnp.abs(step_in)))
    decay = jnp.exp(-step * jnp.exp(decay_log_ref[...]))

    loads[0].wait()
    inner_pre = dot(normed, inner_w[...]).astype(BF16).astype(F32)
    kern = inner_kernel_ref[...]
    conv = inner_pre * kern[3:4]
    for j in range(3):
        conv = conv + inner_window_ref[j].astype(F32) * kern[j : j + 1]
    inner = jax.nn.silu(conv)
    new_inner_ref[0:2] = inner_window_ref[1:3]
    new_inner_ref[2] = inner_pre.astype(BF16)

    loads[1].wait()
    vectors = []
    pres = []
    for r in range(2):
        pre = dot(normed, state_w[r]).astype(BF16).astype(F32)
        conv = pre * state_kernel_ref[3, r : r + 1, :]
        for j in range(3):
            conv = conv + state_window_ref[:, j, r, :].astype(F32) * state_kernel_ref[j, r : r + 1, :]
        vectors.append(jax.nn.silu(conv))
        pres.append(pre)
    new_state_window_ref[:, 0:2] = state_window_ref[:, 1:3]
    new_state_window_ref[:, 2] = jnp.concatenate(
        [pres[0][:, None, :], pres[1][:, None, :]], axis=1
    ).astype(BF16)
    in_vector, out_vector = vectors

    loads[2].wait()
    gate_pre = dot(normed, gate_w[...])

    lane = lax.broadcasted_iota(jnp.int32, inner.shape, 1) // HEAD_DIM
    step_wide = jnp.broadcast_to(step[:, 0:1], inner.shape)
    skip_wide = jnp.broadcast_to(skip_ref[:, 0:1], inner.shape)
    for h in range(1, heads):
        step_wide = jnp.where(lane == h, step[:, h : h + 1], step_wide)
        skip_wide = jnp.where(lane == h, skip_ref[:, h : h + 1], skip_wide)
    for h in range(heads):
        decay_rows[:, h * STATE_DIM : (h + 1) * STATE_DIM] = jnp.broadcast_to(
            decay[:, h : h + 1], (seqs, STATE_DIM)
        )
    spare = jnp.zeros((32 - seqs, inner.shape[1]), F32)
    high, low = two_terms(jnp.concatenate([step_wide * inner, spare], axis=0))
    written = jnp.transpose(
        jnp.concatenate([high, high, low, jnp.zeros_like(low)], axis=0)
    ).astype(BF16)
    spare = spare[:, :STATE_DIM]
    high, low = two_terms(jnp.concatenate([in_vector, spare], axis=0))
    inputs = jnp.concatenate([high, low, high, jnp.zeros_like(low)], axis=0)
    owner = lax.broadcasted_iota(jnp.int32, inputs.shape, 0) % 32
    high, low = two_terms(jnp.concatenate([out_vector, spare], axis=0))
    reader = jnp.concatenate([high, low, jnp.zeros((64, STATE_DIM), F32)], axis=0).astype(BF16)
    reader = jnp.concatenate([reader, reader], axis=1)
    column = lax.broadcasted_iota(jnp.int32, (heads * HEAD_DIM, STATE_DIM), 1) % 32

    stores = []
    for k in range(4):
        state_loads[k].wait()

        def update(i, carry):
            b = k * chunk + i
            added = dot(written, jnp.where(owner == b, inputs, 0.0).astype(BF16))
            rates = decay_rows[pl.ds(b, 1), :]
            news = []
            for h in range(heads):
                new = state[b, h] * rates[:, h * STATE_DIM : (h + 1) * STATE_DIM] + (
                    added[h * HEAD_DIM : (h + 1) * HEAD_DIM]
                )
                state[b, h] = new
                news.append(new)
            new = jnp.concatenate(news, axis=0)
            high = new.astype(BF16)
            both = jnp.concatenate([high, (new - high.astype(F32)).astype(BF16)], axis=1)
            read[...] = jnp.where(column == b, dot_rows(both, reader), read[...])
            return carry

        lax.fori_loop(0, chunk, update, 0, unroll=True)
        store = pltpu.make_async_copy(
            state.at[pl.ds(k * chunk, chunk)], new_state_hbm.at[pl.ds(k * chunk, chunk)], out_sems.at[k]
        )
        store.start()
        stores.append(store)
    mixed = jnp.transpose(read[...])
    mixed_rows = mixed[:seqs] + mixed[32 : 32 + seqs]
    mixed_rows = mixed_rows + skip_wide * inner
    gated = mixed_rows * jax.nn.silu(gate_pre)
    rows = (rms_scale(gated, 1.0) * group_gain_ref[...]).astype(BF16)
    loads[3].wait()
    partial_ref[...] = dot(rows, output_w[...]).astype(BF16)
    for store in stores:
        store.wait()


def ffn_kernel(
    n_ep,
    n_tp,
    partial_ref,
    tokens_ref,
    gain_ref,
    routes_ref,
    route_weights_ref,
    dense_gate_ref,
    dense_up_ref,
    dense_down_ref,
    dense_scale_ref,
    gate_hbm,
    up_hbm,
    down_hbm,
    out_ref,
    w_gate,
    w_up,
    w_down,
    parts,
    residual_ref,
    ffn_ref,
    dw,
    dx,
    combine_ref,
    tall,
    going,
    came,
    xs,
    act,
    dz_going,
    dz_came,
    hid,
    moe_going,
    moe_came,
    tall_back,
    back_going,
    back_came,
    od_going,
    od_came,
    local_sems,
    send_sems,
    recv_sems,
):
    me = lax.axis_index("ep")
    t = lax.axis_index("tp")
    n_z = n_ep // NYC
    z = me // NYC
    yc = me % NYC
    seqs = tokens_ref.shape[0]
    width = out_ref.shape[1]
    slots = 2 * n_ep

    def across_tp(k):
        return (me, lax.rem(t + k, n_tp))

    def along_z(k):
        return (lax.rem(z + k, n_z) * NYC + yc, t)

    def within_z(k):
        return (z * NYC + lax.rem(yc + k, NYC), t)

    def along_ep(kz, k):
        return (lax.rem(z + kz, n_z) * NYC + lax.rem(yc + k, NYC), t)

    steps = sorted(range(n_z), key=lambda kz: -min(kz, n_z - kz))

    def to_all(send):
        for kz in steps:
            for k in range(0 if kz else 1, NYC):
                send(along_ep(kz, k))

    def remote(src, dst, which, peer):
        return pltpu.make_async_remote_copy(
            src_ref=src,
            dst_ref=dst,
            send_sem=send_sems.at[which],
            recv_sem=recv_sems.at[which],
            device_id=peer,
            device_id_type=MESH,
        )

    def wait_in(ref, which):
        remote(ref, ref, which, across_tp(1)).wait_recv()

    def wait_out(ref, which):
        remote(ref, ref, which, across_tp(1)).wait_send()

    PART, DW, DW2, DX, OUT, DZ, HID, MOE, BACK, OD = range(10)

    barrier = pltpu.get_barrier_semaphore()
    for k in range(1, n_tp):
        pl.semaphore_signal(barrier, inc=1, device_id=across_tp(k), device_id_type=MESH)

    to_all(
        lambda peer: pl.semaphore_signal(barrier, inc=1, device_id=peer, device_id_type=MESH)
    )

    loads = [
        pltpu.make_async_copy(src.at[0], dst, local_sems.at[i])
        for i, (src, dst) in enumerate([(gate_hbm, w_gate), (up_hbm, w_up), (down_hbm, w_down)])
    ]
    for load in loads:
        load.start()

    units = dense_gate_ref.shape[0]
    gap = jnp.zeros((UNITS - units, width), F32)
    for i, ref in enumerate((dense_gate_ref, dense_up_ref, dense_down_ref)):
        dw[yc, i * UNITS : (i + 1) * UNITS] = jnp.concatenate(
            [ref[...].astype(F32), gap], axis=0
        ).astype(BF16)
    parts[t] = partial_ref[...]

    expert = lax.broadcasted_iota(jnp.int32, (n_ep, seqs), 0)
    named = [(routes_ref[k : k + 1, :] == expert).astype(F32) for k in range(2)]
    earlier = (
        lax.broadcasted_iota(jnp.int32, (seqs, seqs), 0)
        < lax.broadcasted_iota(jnp.int32, (seqs, seqs), 1)
    ).astype(F32)
    before = dot(named[0] + named[1], earlier)
    place = lax.broadcasted_iota(jnp.int32, (slots, seqs), 0)
    chosen = []
    for k in range(2):
        slot = jnp.sum(before * named[k], axis=0, keepdims=True).astype(jnp.int32)
        chosen.append((place == routes_ref[k : k + 1, :] * 2 + slot).astype(F32))
    selection = (chosen[0] + chosen[1]).astype(BF16)
    combine_ref[...] = jnp.transpose(
        chosen[0] * route_weights_ref[0:1, :] + chosen[1] * route_weights_ref[1:2, :]
    )

    pl.semaphore_wait(barrier, n_tp - 1 + n_ep - 1)

    for k in range(1, n_tp):
        remote(partial_ref, parts.at[t], PART, across_tp(k)).start()

    for k in range(2, NYC, 2):
        remote(dw.at[yc], dw.at[yc], DW, within_z(k)).start()

    wait_in(parts.at[pl.ds(0, n_tp - 1)], PART)
    total = parts[0].astype(F32)
    for k in range(1, n_tp):
        total = total + parts[k].astype(F32)
    residual = tokens_ref[...].astype(F32) + total
    residual_ref[...] = residual
    ffn = rms_scale(residual, gain_ref[...]).astype(BF16)
    ffn_ref[...] = ffn

    own = pl.ds(pl.multiple_of(t * width, width), width)
    dx[z] = ffn_ref[:, own]

    for k in steps[:-1]:
        remote(dx.at[z], dx.at[z], DX, along_z(k)).start()

    outgoing = dot(selection, ffn)
    lines = outgoing.shape[1] // 128
    for j in range(lines):
        tall[pl.ds(j, slots, stride=lines), :] = outgoing[:, j * 128 : (j + 1) * 128]
    going[...] = tall[...].reshape(going.shape).astype(BF16)

    to_all(lambda peer: remote(going.at[peer[0]], came.at[me], OUT, peer).start())
    came[me] = going[me]

    wait_in(dw.at[pl.ds(0, NYC // 2 - 1)], DW)
    sibling = (z * NYC + yc + 1 - 2 * lax.rem(yc, 2), t)
    for k in range(0, NYC, 2):
        held = lax.rem(yc + k, NYC)
        remote(dw.at[held], dw.at[held], DW2, sibling).start()
    wait_in(dw.at[pl.ds(0, NYC // 2)], DW2)
    wait_in(dx.at[pl.ds(0, n_z - 1)], DX)
    dense_rows = dx[...].reshape(n_z * seqs, width)
    for i in range(2):
        weights = dw[:, i * UNITS : (i + 1) * UNITS].reshape(NYC * UNITS, width)
        dz_going[:, :, i * NYC * UNITS : (i + 1) * NYC * UNITS] = (
            dot_rows(dense_rows, weights).astype(BF16).reshape(n_tp, -1, NYC * UNITS)
        )
    for k in range(1, n_tp):
        peer = across_tp(k)
        remote(dz_going.at[peer[1]], dz_came.at[t], DZ, peer).start()
    dz_came[t] = dz_going[t]

    wait_in(came.at[pl.ds(0, n_ep - 1)], OUT)
    tall[...] = came[...].astype(F32).reshape(tall.shape)
    for j in range(lines):
        xs[:, j * 128 : (j + 1) * 128] = tall[pl.ds(j, slots, stride=lines), :].astype(BF16)
    loads[0].wait()
    loads[1].wait()
    rows = xs[...]
    act[...] = (jax.nn.silu(dot_rows(rows, w_gate[...])) * dot_rows(rows, w_up[...])).astype(BF16)
    loads[2].wait()
    for k in range(1, n_tp):
        peer = across_tp(k)
        columns = pl.ds(pl.multiple_of(peer[1] * width, width), width)
        moe_going[peer[1]] = dot(act[...], w_down[:, columns]).astype(BF16)
        remote(moe_going.at[peer[1]], moe_came.at[t], MOE, peer).start()
    moe_came[t] = dot(act[...], w_down[:, own]).astype(BF16)

    wait_in(dz_came.at[pl.ds(0, n_tp - 1)], DZ)
    gate_up = dz_came[0].astype(F32)
    for k in range(1, n_tp):
        gate_up = gate_up + dz_came[k].astype(F32)
    hid[t] = (
        jax.nn.silu(gate_up[:, : NYC * UNITS]) * gate_up[:, NYC * UNITS :]
    ).astype(BF16)
    for k in range(1, n_tp):
        remote(hid.at[t], hid.at[t], HID, across_tp(k)).start()

    wait_in(moe_came.at[pl.ds(0, n_tp - 1)], MOE)
    rows_out = moe_came[0].astype(F32)
    for k in range(1, n_tp):
        rows_out = rows_out + moe_came[k].astype(F32)
    for j in range(width // 128):
        tall_back[pl.ds(j, slots, stride=4), :] = rows_out[:, j * 128 : (j + 1) * 128]
    back_going[...] = tall_back[...].reshape(back_going.shape).astype(BF16)

    to_all(lambda peer: remote(back_going.at[peer[0]], back_came.at[me], BACK, peer).start())
    back_came[me] = back_going[me]

    wait_in(hid.at[pl.ds(0, n_tp - 1)], HID)
    dense_part = dot(
        hid[...].reshape(n_z * seqs, NYC * UNITS),
        dw[:, 2 * UNITS : 3 * UNITS].reshape(NYC * UNITS, width),
    )
    od_going[...] = dense_part.astype(BF16).reshape(od_going.shape)

    for k in steps[:-1]:
        there = lax.rem(z + k, n_z)
        remote(od_going.at[there], od_came.at[z], OD, along_z(k)).start()
    od_came[z] = od_going[z]

    wait_in(od_came.at[pl.ds(0, n_z - 1)], OD)
    dense_out = od_came[0].astype(F32)
    for k in range(1, n_z):
        dense_out = dense_out + od_came[k].astype(F32)

    wait_in(back_came.at[pl.ds(0, n_ep - 1)], BACK)
    tall_back[...] = back_came[...].astype(F32).reshape(tall_back.shape)
    returned = [
        tall_back[pl.ds(j, slots, stride=4), :].astype(BF16) for j in range(width // 128)
    ]
    returned = jnp.concatenate(returned, axis=1).astype(F32)
    expert_out = jnp.dot(combine_ref[...], returned, precision=lax.Precision.HIGHEST)
    out_ref[...] = (
        residual_ref[:, own] + expert_out + dense_scale_ref[...] * dense_out
    ).astype(BF16)

    wait_out(parts.at[pl.ds(0, n_tp - 1)], PART)
    wait_out(dw.at[pl.ds(0, NYC // 2 - 1)], DW)
    wait_out(dw.at[pl.ds(0, NYC // 2)], DW2)
    wait_out(dx.at[pl.ds(0, n_z - 1)], DX)
    wait_out(going.at[pl.ds(0, n_ep - 1)], OUT)
    wait_out(dz_going.at[pl.ds(0, n_tp - 1)], DZ)
    wait_out(hid.at[pl.ds(0, n_tp - 1)], HID)
    wait_out(moe_going.at[pl.ds(0, n_tp - 1)], MOE)
    wait_out(back_going.at[pl.ds(0, n_ep - 1)], BACK)
    wait_out(od_going.at[pl.ds(0, n_z - 1)], OD)


VMEM = pl.BlockSpec(memory_space=pltpu.VMEM)
ANY = pl.BlockSpec(memory_space=pl.ANY)


def local(
    n_ep,
    n_tp,
    tokens,
    mixer_gain,
    gate_weight,
    inner_weight,
    state_weight,
    step_weight,
    step_bias,
    decay_log,
    skip_scale,
    inner_kernel,
    state_kernel,
    inner_window,
    state_window,
    recurrent_state,
    group_gain,
    output_weight,
    channel_gain,
    routes,
    route_weights,
    expert_gate,
    expert_up,
    expert_down,
    dense_gate,
    dense_up,
    dense_down,
    dense_scale,
):
    seqs, model = tokens.shape
    width = dense_scale.shape[0]
    hidden = expert_gate.shape[2]
    n_z = n_ep // NYC
    slots = 2 * n_ep
    sds = jax.ShapeDtypeStruct
    partial, new_inner, new_window, new_state = pl.pallas_call(
        mixer_kernel,
        out_shape=(
            sds((seqs, model), BF16),
            sds((3, seqs, width), BF16),
            sds(state_window.shape, BF16),
            sds(recurrent_state.shape, F32),
        ),
        in_specs=[VMEM] * 11 + [ANY] * 5,
        out_specs=(VMEM, VMEM, VMEM, ANY),
        scratch_shapes=[
            pltpu.VMEM(gate_weight.shape, BF16),
            pltpu.VMEM(inner_weight.shape, BF16),
            pltpu.VMEM(state_weight.shape, BF16),
            pltpu.VMEM(output_weight.shape, BF16),
            pltpu.VMEM(recurrent_state.shape, F32),
            pltpu.VMEM((seqs, step_bias.shape[0] * STATE_DIM), F32),
            pltpu.VMEM((width, STATE_DIM), F32),
            pltpu.SemaphoreType.DMA((4,)),
            pltpu.SemaphoreType.DMA((4,)),
            pltpu.SemaphoreType.DMA((4,)),
        ],
        name="mixer",
    )(
        tokens,
        mixer_gain[None],
        step_weight.T,
        step_bias[None],
        decay_log[None],
        skip_scale[None],
        inner_kernel,
        state_kernel,
        jnp.swapaxes(inner_window, 0, 1),
        state_window,
        group_gain[None],
        gate_weight,
        inner_weight,
        state_weight,
        output_weight,
        recurrent_state,
    )
    scratch = [
        pltpu.VMEM((hidden, model), BF16),
        pltpu.VMEM((hidden, model), BF16),
        pltpu.VMEM((hidden, model), BF16),
        pltpu.VMEM((n_tp, seqs, model), BF16),
        pltpu.VMEM((seqs, model), F32),
        pltpu.VMEM((seqs, model), BF16),
        pltpu.VMEM((NYC, 3 * UNITS, width), BF16),
        pltpu.VMEM((n_z, seqs, width), BF16),
        pltpu.VMEM((seqs, slots), F32),
        pltpu.VMEM((slots * model // 128, 128), F32),
        pltpu.VMEM((n_ep, 2 * model // 128, 128), BF16),
        pltpu.VMEM((n_ep, 2 * model // 128, 128), BF16),
        pltpu.VMEM((slots, model), BF16),
        pltpu.VMEM((slots, hidden), BF16),
        pltpu.VMEM((n_tp, n_z * seqs // n_tp, 2 * NYC * UNITS), BF16),
        pltpu.VMEM((n_tp, n_z * seqs // n_tp, 2 * NYC * UNITS), BF16),
        pltpu.VMEM((n_tp, n_z * seqs // n_tp, NYC * UNITS), BF16),
        pltpu.VMEM((n_tp, slots, width), BF16),
        pltpu.VMEM((n_tp, slots, width), BF16),
        pltpu.VMEM((slots * 4, 128), F32),
        pltpu.VMEM((n_ep, 8, 128), BF16),
        pltpu.VMEM((n_ep, 8, 128), BF16),
        pltpu.VMEM((n_z, seqs, width), BF16),
        pltpu.VMEM((n_z, seqs, width), BF16),
        pltpu.SemaphoreType.DMA((3,)),
        pltpu.SemaphoreType.DMA((10,)),
        pltpu.SemaphoreType.DMA((10,)),
    ]
    new_tokens = pl.pallas_call(
        functools.partial(ffn_kernel, n_ep, n_tp),
        out_shape=sds((seqs, width), BF16),
        in_specs=[VMEM] * 9 + [ANY] * 3,
        out_specs=VMEM,
        scratch_shapes=scratch,
        compiler_params=pltpu.CompilerParams(collective_id=0, has_side_effects=True),
        name="ffn",
    )(
        partial,
        tokens,
        channel_gain[None],
        routes.T,
        route_weights.T,
        dense_gate.T,
        dense_up.T,
        dense_down,
        dense_scale[None],
        jnp.swapaxes(expert_gate, 1, 2),
        jnp.swapaxes(expert_up, 1, 2),
        expert_down,
    )
    return new_tokens, new_state, jnp.swapaxes(new_inner, 0, 1), new_window


def solution(mesh):
    placed = (
        P("ep", None),
        P(),
        P(None, "tp"),
        P(None, "tp"),
        P(None, None, "tp"),
        P(None, "tp"),
        P("tp"),
        P("tp"),
        P("tp"),
        P(None, "tp"),
        P(None, None, "tp"),
        P("ep", None, "tp"),
        P("ep", None, None, "tp"),
        P("ep", "tp", None, None),
        P("tp"),
        P("tp", None),
        P(),
        P("ep", None),
        P("ep", None),
        P("ep", None, "tp"),
        P("ep", None, "tp"),
        P("ep", "tp", None),
        P("tp", "ep"),
        P("tp", "ep"),
        P("ep", "tp"),
        P("tp"),
    )
    return jax.shard_map(
        functools.partial(local, mesh.shape["ep"], mesh.shape["tp"]),
        mesh=mesh,
        in_specs=placed,
        out_specs=(
            P("ep", "tp"),
            P("ep", "tp", None, None),
            P("ep", None, "tp"),
            P("ep", None, None, "tp"),
        ),
        check_vma=False,
    )
```

```python
import functools

import jax
import jax.numpy as jnp
from jax import lax
from jax.experimental import pallas as pl
from jax.experimental.pallas import tpu as pltpu
from jax.sharding import PartitionSpec as P

MESH = pl.DeviceIdType.MESH
F32 = jnp.float32
BF16 = jnp.bfloat16
HEAD_DIM = 64
STATE_DIM = 128
NYC = 8
UNITS = 48
eps = 1e-06


def rms_scale(values, norm_gain):
    squares = jnp.mean(values * values, axis=-1, keepdims=True)
    return values * lax.rsqrt(squares + eps) * norm_gain


def dot(a, b):
    return jnp.dot(a, b, preferred_element_type=F32)


def two_terms(v):
    high = v.astype(BF16).astype(F32)
    return high, (v - high).astype(BF16).astype(F32)


def dot_rows(a, b):
    return lax.dot_general(a, b, (((1,), (1,)), ((), ())), preferred_element_type=F32)


def layer_kernel(
    n_ep,
    n_tp,
    tokens_ref,
    mixer_gain_ref,
    step_weight_ref,
    step_bias_ref,
    decay_log_ref,
    skip_ref,
    inner_kernel_ref,
    state_kernel_ref,
    inner_window_ref,
    state_window_ref,
    group_gain_ref,
    gain_ref,
    routes_ref,
    route_weights_ref,
    dense_gate_ref,
    dense_up_ref,
    dense_down_ref,
    dense_scale_ref,
    gate_weight_hbm,
    inner_weight_hbm,
    state_weight_hbm,
    output_weight_hbm,
    state_hbm,
    gate_hbm,
    up_hbm,
    down_hbm,
    out_ref,
    new_inner_ref,
    new_state_window_ref,
    new_state_ref,
    gate_w,
    inner_w,
    state_w,
    output_w,
    decay_rows,
    read,
    w_gate,
    w_up,
    w_down,
    parts,
    residual_ref,
    ffn_ref,
    dw,
    dx,
    combine_ref,
    tall,
    going,
    came,
    xs,
    act,
    dz_going,
    dz_came,
    hid,
    moe_going,
    moe_came,
    tall_back,
    back_going,
    back_came,
    od_going,
    od_came,
    in_sems,
    state_sems,
    local_sems,
    send_sems,
    recv_sems,
):
    me = lax.axis_index("ep")
    t = lax.axis_index("tp")
    n_z = n_ep // NYC
    z = me // NYC
    yc = me % NYC
    seqs = tokens_ref.shape[0]
    heads = new_state_ref.shape[1]
    chunk = seqs // 4
    width = out_ref.shape[1]
    slots = 2 * n_ep

    def across_tp(k):
        return (me, lax.rem(t + k, n_tp))

    def along_z(k):
        return (lax.rem(z + k, n_z) * NYC + yc, t)

    def within_z(k):
        return (z * NYC + lax.rem(yc + k, NYC), t)

    def along_ep(kz, k):
        return (lax.rem(z + kz, n_z) * NYC + lax.rem(yc + k, NYC), t)

    steps = sorted(range(n_z), key=lambda kz: -min(kz, n_z - kz))

    def to_all(send):
        for kz in steps:
            for k in range(0 if kz else 1, NYC):
                send(along_ep(kz, k))

    def remote(src, dst, which, peer):
        return pltpu.make_async_remote_copy(
            src_ref=src,
            dst_ref=dst,
            send_sem=send_sems.at[which],
            recv_sem=recv_sems.at[which],
            device_id=peer,
            device_id_type=MESH,
        )

    def wait_in(ref, which):
        remote(ref, ref, which, across_tp(1)).wait_recv()

    def wait_out(ref, which):
        remote(ref, ref, which, across_tp(1)).wait_send()

    PART, DW, DW2, DX, OUT, DZ, HID, MOE, BACK, OD = range(10)

    mixer_loads = [
        pltpu.make_async_copy(src, dst, in_sems.at[i])
        for i, (src, dst) in enumerate(
            [
                (inner_weight_hbm, inner_w),
                (state_weight_hbm, state_w),
                (gate_weight_hbm, gate_w),
                (output_weight_hbm, output_w),
            ]
        )
    ]
    for load in mixer_loads[:3]:
        load.start()
    state_loads = [
        pltpu.make_async_copy(
            state_hbm.at[pl.ds(c * chunk, chunk)], new_state_ref.at[pl.ds(c * chunk, chunk)], state_sems.at[c]
        )
        for c in range(4)
    ]
    for load in state_loads:
        load.start()
    mixer_loads[3].start()


    barrier = pltpu.get_barrier_semaphore()
    for k in range(1, n_tp):
        pl.semaphore_signal(barrier, inc=1, device_id=across_tp(k), device_id_type=MESH)

    to_all(
        lambda peer: pl.semaphore_signal(barrier, inc=1, device_id=peer, device_id_type=MESH)
    )

    loads = [
        pltpu.make_async_copy(src.at[0], dst, local_sems.at[i])
        for i, (src, dst) in enumerate([(gate_hbm, w_gate), (up_hbm, w_up), (down_hbm, w_down)])
    ]
    for load in loads:
        load.start()

    units = dense_gate_ref.shape[0]
    gap = jnp.zeros((UNITS - units, width), F32)
    for i, ref in enumerate((dense_gate_ref, dense_up_ref, dense_down_ref)):
        dw[yc, i * UNITS : (i + 1) * UNITS] = jnp.concatenate(
            [ref[...].astype(F32), gap], axis=0
        ).astype(BF16)

    expert = lax.broadcasted_iota(jnp.int32, (n_ep, seqs), 0)
    named = [(routes_ref[k : k + 1, :] == expert).astype(F32) for k in range(2)]
    earlier = (
        lax.broadcasted_iota(jnp.int32, (seqs, seqs), 0)
        < lax.broadcasted_iota(jnp.int32, (seqs, seqs), 1)
    ).astype(F32)
    before = dot(named[0] + named[1], earlier)
    place = lax.broadcasted_iota(jnp.int32, (slots, seqs), 0)
    chosen = []
    for k in range(2):
        slot = jnp.sum(before * named[k], axis=0, keepdims=True).astype(jnp.int32)
        chosen.append((place == routes_ref[k : k + 1, :] * 2 + slot).astype(F32))
    selection = (chosen[0] + chosen[1]).astype(BF16)
    combine_ref[...] = jnp.transpose(
        chosen[0] * route_weights_ref[0:1, :] + chosen[1] * route_weights_ref[1:2, :]
    )

    normed = rms_scale(tokens_ref[...].astype(F32), mixer_gain_ref[...]).astype(BF16)
    step_raw = dot_rows(normed, step_weight_ref[...])
    step_in = step_raw + step_bias_ref[...]
    step = jnp.maximum(step_in, 0.0) + jnp.log1p(jnp.exp(-jnp.abs(step_in)))
    decay = jnp.exp(-step * jnp.exp(decay_log_ref[...]))

    mixer_loads[0].wait()
    inner_pre = dot(normed, inner_w[...]).astype(BF16).astype(F32)
    kern = inner_kernel_ref[...]
    conv = inner_pre * kern[3:4]
    for j in range(3):
        conv = conv + inner_window_ref[j].astype(F32) * kern[j : j + 1]
    inner = jax.nn.silu(conv)
    new_inner_ref[0:2] = inner_window_ref[1:3]
    new_inner_ref[2] = inner_pre.astype(BF16)

    mixer_loads[1].wait()
    vectors = []
    pres = []
    for r in range(2):
        pre = dot(normed, state_w[r]).astype(BF16).astype(F32)
        conv = pre * state_kernel_ref[3, r : r + 1, :]
        for j in range(3):
            conv = conv + state_window_ref[:, j, r, :].astype(F32) * state_kernel_ref[j, r : r + 1, :]
        vectors.append(jax.nn.silu(conv))
        pres.append(pre)
    new_state_window_ref[:, 0:2] = state_window_ref[:, 1:3]
    new_state_window_ref[:, 2] = jnp.concatenate(
        [pres[0][:, None, :], pres[1][:, None, :]], axis=1
    ).astype(BF16)
    in_vector, out_vector = vectors

    mixer_loads[2].wait()
    gate_pre = dot(normed, gate_w[...])

    lane = lax.broadcasted_iota(jnp.int32, inner.shape, 1) // HEAD_DIM
    step_wide = jnp.broadcast_to(step[:, 0:1], inner.shape)
    skip_wide = jnp.broadcast_to(skip_ref[:, 0:1], inner.shape)
    for h in range(1, heads):
        step_wide = jnp.where(lane == h, step[:, h : h + 1], step_wide)
        skip_wide = jnp.where(lane == h, skip_ref[:, h : h + 1], skip_wide)
    for h in range(heads):
        decay_rows[:, h * STATE_DIM : (h + 1) * STATE_DIM] = jnp.broadcast_to(
            decay[:, h : h + 1], (seqs, STATE_DIM)
        )
    spare = jnp.zeros((32 - seqs, inner.shape[1]), F32)
    high, low = two_terms(jnp.concatenate([step_wide * inner, spare], axis=0))
    written = jnp.transpose(
        jnp.concatenate([high, high, low, jnp.zeros_like(low)], axis=0)
    ).astype(BF16)
    spare = spare[:, :STATE_DIM]
    high, low = two_terms(jnp.concatenate([in_vector, spare], axis=0))
    inputs = jnp.concatenate([high, low, high, jnp.zeros_like(low)], axis=0)
    owner = lax.broadcasted_iota(jnp.int32, inputs.shape, 0) % 32
    high, low = two_terms(jnp.concatenate([out_vector, spare], axis=0))
    reader = jnp.concatenate([high, low, jnp.zeros((64, STATE_DIM), F32)], axis=0).astype(BF16)
    reader = jnp.concatenate([reader, reader], axis=1)
    column = lax.broadcasted_iota(jnp.int32, (heads * HEAD_DIM, STATE_DIM), 1) % 32

    for k in range(4):
        state_loads[k].wait()

        def update(i, carry):
            b = k * chunk + i
            added = dot(written, jnp.where(owner == b, inputs, 0.0).astype(BF16))
            rates = decay_rows[pl.ds(b, 1), :]
            news = []
            for h in range(heads):
                new = new_state_ref[b, h] * rates[:, h * STATE_DIM : (h + 1) * STATE_DIM] + (
                    added[h * HEAD_DIM : (h + 1) * HEAD_DIM]
                )
                new_state_ref[b, h] = new
                news.append(new)
            new = jnp.concatenate(news, axis=0)
            high = new.astype(BF16)
            both = jnp.concatenate([high, (new - high.astype(F32)).astype(BF16)], axis=1)
            read[...] = jnp.where(column == b, dot_rows(both, reader), read[...])
            return carry

        lax.fori_loop(0, chunk, update, 0, unroll=True)
    mixed = jnp.transpose(read[...])
    mixed_rows = mixed[:seqs] + mixed[32 : 32 + seqs]
    mixed_rows = mixed_rows + skip_wide * inner
    gated = mixed_rows * jax.nn.silu(gate_pre)
    mixer_rows = (rms_scale(gated, 1.0) * group_gain_ref[...]).astype(BF16)
    mixer_loads[3].wait()
    parts[t] = dot(mixer_rows, output_w[...]).astype(BF16)

    pl.semaphore_wait(barrier, n_tp - 1 + n_ep - 1)

    for k in range(1, n_tp):
        remote(parts.at[t], parts.at[t], PART, across_tp(k)).start()

    for k in range(2, NYC, 2):
        remote(dw.at[yc], dw.at[yc], DW, within_z(k)).start()

    wait_in(parts.at[pl.ds(0, n_tp - 1)], PART)
    total = parts[0].astype(F32)
    for k in range(1, n_tp):
        total = total + parts[k].astype(F32)
    residual = tokens_ref[...].astype(F32) + total
    residual_ref[...] = residual
    ffn = rms_scale(residual, gain_ref[...]).astype(BF16)
    ffn_ref[...] = ffn

    own = pl.ds(pl.multiple_of(t * width, width), width)
    dx[z] = ffn_ref[:, own]

    for k in steps[:-1]:
        remote(dx.at[z], dx.at[z], DX, along_z(k)).start()

    outgoing = dot(selection, ffn)
    lines = outgoing.shape[1] // 128
    for j in range(lines):
        tall[pl.ds(j, slots, stride=lines), :] = outgoing[:, j * 128 : (j + 1) * 128]
    going[...] = tall[...].reshape(going.shape).astype(BF16)

    to_all(lambda peer: remote(going.at[peer[0]], came.at[me], OUT, peer).start())
    came[me] = going[me]

    wait_in(dw.at[pl.ds(0, NYC // 2 - 1)], DW)
    sibling = (z * NYC + yc + 1 - 2 * lax.rem(yc, 2), t)
    for k in range(0, NYC, 2):
        held = lax.rem(yc + k, NYC)
        remote(dw.at[held], dw.at[held], DW2, sibling).start()
    wait_in(dw.at[pl.ds(0, NYC // 2)], DW2)
    wait_in(dx.at[pl.ds(0, n_z - 1)], DX)
    dense_rows = dx[...].reshape(n_z * seqs, width)
    for i in range(2):
        weights = dw[:, i * UNITS : (i + 1) * UNITS].reshape(NYC * UNITS, width)
        dz_going[:, :, i * NYC * UNITS : (i + 1) * NYC * UNITS] = (
            dot_rows(dense_rows, weights).astype(BF16).reshape(n_tp, -1, NYC * UNITS)
        )
    for k in range(1, n_tp):
        peer = across_tp(k)
        remote(dz_going.at[peer[1]], dz_came.at[t], DZ, peer).start()
    dz_came[t] = dz_going[t]

    wait_in(came.at[pl.ds(0, n_ep - 1)], OUT)
    wait_in(dz_came.at[pl.ds(0, n_tp - 1)], DZ)
    gate_up = dz_came[0].astype(F32)
    for k in range(1, n_tp):
        gate_up = gate_up + dz_came[k].astype(F32)
    hid[t] = (
        jax.nn.silu(gate_up[:, : NYC * UNITS]) * gate_up[:, NYC * UNITS :]
    ).astype(BF16)
    for k in range(1, n_tp):
        remote(hid.at[t], hid.at[t], HID, across_tp(k)).start()

    tall[...] = came[...].astype(F32).reshape(tall.shape)
    for j in range(lines):
        xs[:, j * 128 : (j + 1) * 128] = tall[pl.ds(j, slots, stride=lines), :].astype(BF16)
    loads[0].wait()
    loads[1].wait()
    rows = xs[...]
    act[...] = (jax.nn.silu(dot_rows(rows, w_gate[...])) * dot_rows(rows, w_up[...])).astype(BF16)
    loads[2].wait()
    for k in range(1, n_tp):
        peer = across_tp(k)
        columns = pl.ds(pl.multiple_of(peer[1] * width, width), width)
        moe_going[peer[1]] = dot(act[...], w_down[:, columns]).astype(BF16)
        remote(moe_going.at[peer[1]], moe_came.at[t], MOE, peer).start()
    moe_came[t] = dot(act[...], w_down[:, own]).astype(BF16)

    wait_in(hid.at[pl.ds(0, n_tp - 1)], HID)
    dense_part = dot(
        hid[...].reshape(n_z * seqs, NYC * UNITS),
        dw[:, 2 * UNITS : 3 * UNITS].reshape(NYC * UNITS, width),
    )
    od_going[...] = dense_part.astype(BF16).reshape(od_going.shape)

    for k in steps[:-1]:
        there = lax.rem(z + k, n_z)
        remote(od_going.at[there], od_came.at[z], OD, along_z(k)).start()
    od_came[z] = od_going[z]

    wait_in(moe_came.at[pl.ds(0, n_tp - 1)], MOE)
    rows_out = moe_came[0].astype(F32)
    for k in range(1, n_tp):
        rows_out = rows_out + moe_came[k].astype(F32)
    for j in range(width // 128):
        tall_back[pl.ds(j, slots, stride=2), :] = rows_out[:, j * 128 : (j + 1) * 128]
    back_going[...] = tall_back[...].reshape(back_going.shape).astype(BF16)

    to_all(lambda peer: remote(back_going.at[peer[0]], back_came.at[me], BACK, peer).start())
    back_came[me] = back_going[me]

    wait_in(od_came.at[pl.ds(0, n_z - 1)], OD)
    dense_out = od_came[0].astype(F32)
    for k in range(1, n_z):
        dense_out = dense_out + od_came[k].astype(F32)

    wait_in(back_came.at[pl.ds(0, n_ep - 1)], BACK)
    tall_back[...] = back_came[...].astype(F32).reshape(tall_back.shape)
    returned = [
        tall_back[pl.ds(j, slots, stride=2), :].astype(BF16) for j in range(width // 128)
    ]
    returned = jnp.concatenate(returned, axis=1).astype(F32)
    expert_out = jnp.dot(combine_ref[...], returned, precision=lax.Precision.HIGHEST)
    out_ref[...] = (
        residual_ref[:, own] + expert_out + dense_scale_ref[...] * dense_out
    ).astype(BF16)

    wait_out(parts.at[pl.ds(0, n_tp - 1)], PART)
    wait_out(dw.at[pl.ds(0, NYC // 2 - 1)], DW)
    wait_out(dw.at[pl.ds(0, NYC // 2)], DW2)
    wait_out(dx.at[pl.ds(0, n_z - 1)], DX)
    wait_out(going.at[pl.ds(0, n_ep - 1)], OUT)
    wait_out(dz_going.at[pl.ds(0, n_tp - 1)], DZ)
    wait_out(hid.at[pl.ds(0, n_tp - 1)], HID)
    wait_out(moe_going.at[pl.ds(0, n_tp - 1)], MOE)
    wait_out(back_going.at[pl.ds(0, n_ep - 1)], BACK)
    wait_out(od_going.at[pl.ds(0, n_z - 1)], OD)


def write_kernel(*refs):
    sems = refs[-1]
    copies = [pltpu.make_async_copy(refs[i], refs[4 + i], sems.at[i]) for i in (3, 0, 1, 2)]
    for copy in copies:
        copy.start()
    for copy in copies:
        copy.wait()


VMEM = pl.BlockSpec(memory_space=pltpu.VMEM)
ANY = pl.BlockSpec(memory_space=pl.ANY)


def local(
    n_ep,
    n_tp,
    tokens,
    mixer_gain,
    gate_weight,
    inner_weight,
    state_weight,
    step_weight,
    step_bias,
    decay_log,
    skip_scale,
    inner_kernel,
    state_kernel,
    inner_window,
    state_window,
    recurrent_state,
    group_gain,
    output_weight,
    channel_gain,
    routes,
    route_weights,
    expert_gate,
    expert_up,
    expert_down,
    dense_gate,
    dense_up,
    dense_down,
    dense_scale,
):
    seqs, model = tokens.shape
    width = dense_scale.shape[0]
    hidden = expert_gate.shape[2]
    n_z = n_ep // NYC
    slots = 2 * n_ep
    scratch = [
        pltpu.VMEM(gate_weight.shape, BF16),
        pltpu.VMEM(inner_weight.shape, BF16),
        pltpu.VMEM(state_weight.shape, BF16),
        pltpu.VMEM(output_weight.shape, BF16),
        pltpu.VMEM((seqs, step_bias.shape[0] * STATE_DIM), F32),
        pltpu.VMEM((width, STATE_DIM), F32),
        pltpu.VMEM((hidden, model), BF16),
        pltpu.VMEM((hidden, model), BF16),
        pltpu.VMEM((hidden, model), BF16),
        pltpu.VMEM((n_tp, seqs, model), BF16),
        pltpu.VMEM((seqs, model), F32),
        pltpu.VMEM((seqs, model), BF16),
        pltpu.VMEM((NYC, 3 * UNITS, width), BF16),
        pltpu.VMEM((n_z, seqs, width), BF16),
        pltpu.VMEM((seqs, slots), F32),
        pltpu.VMEM((slots * model // 128, 128), F32),
        pltpu.VMEM((n_ep, 2 * model // 128, 128), BF16),
        pltpu.VMEM((n_ep, 2 * model // 128, 128), BF16),
        pltpu.VMEM((slots, model), BF16),
        pltpu.VMEM((slots, hidden), BF16),
        pltpu.VMEM((n_tp, n_z * seqs // n_tp, 2 * NYC * UNITS), BF16),
        pltpu.VMEM((n_tp, n_z * seqs // n_tp, 2 * NYC * UNITS), BF16),
        pltpu.VMEM((n_tp, n_z * seqs // n_tp, NYC * UNITS), BF16),
        pltpu.VMEM((n_tp, slots, width), BF16),
        pltpu.VMEM((n_tp, slots, width), BF16),
        pltpu.VMEM((slots * 2, 128), F32),
        pltpu.VMEM((n_ep, 4, 128), BF16),
        pltpu.VMEM((n_ep, 4, 128), BF16),
        pltpu.VMEM((n_z, seqs, width), BF16),
        pltpu.VMEM((n_z, seqs, width), BF16),
        pltpu.SemaphoreType.DMA((4,)),
        pltpu.SemaphoreType.DMA((4,)),
        pltpu.SemaphoreType.DMA((3,)),
        pltpu.SemaphoreType.DMA((10,)),
        pltpu.SemaphoreType.DMA((10,)),
    ]
    results = [
        ((seqs, width), BF16),
        ((3, seqs, width), BF16),
        (state_window.shape, BF16),
        (recurrent_state.shape, F32),
    ]
    held = pl.pallas_call(
        functools.partial(layer_kernel, n_ep, n_tp),
        out_shape=tuple(pltpu.VMEM(*r) for r in results),
        in_specs=[VMEM] * 18 + [ANY] * 8,
        out_specs=(VMEM,) * 4,
        scratch_shapes=scratch,
        compiler_params=pltpu.CompilerParams(collective_id=0, has_side_effects=True),
        name="layer",
    )(
        tokens,
        mixer_gain[None],
        step_weight.T,
        step_bias[None],
        decay_log[None],
        skip_scale[None],
        inner_kernel,
        state_kernel,
        jnp.swapaxes(inner_window, 0, 1),
        state_window,
        group_gain[None],
        channel_gain[None],
        routes.T,
        route_weights.T,
        dense_gate.T,
        dense_up.T,
        dense_down,
        dense_scale[None],
        gate_weight,
        inner_weight,
        state_weight,
        output_weight,
        recurrent_state,
        jnp.swapaxes(expert_gate, 1, 2),
        jnp.swapaxes(expert_up, 1, 2),
        expert_down,
    )
    new_tokens, new_inner, new_window, new_state = pl.pallas_call(
        write_kernel,
        out_shape=tuple(jax.ShapeDtypeStruct(*r) for r in results),
        in_specs=[VMEM] * 4,
        out_specs=(ANY,) * 4,
        scratch_shapes=[pltpu.SemaphoreType.DMA((4,))],
        name="write",
    )(*(pltpu.with_memory_space_constraint(h, pltpu.VMEM) for h in held))
    return new_tokens, new_state, jnp.swapaxes(new_inner, 0, 1), new_window


def solution(mesh):
    placed = (
        P("ep", None),
        P(),
        P(None, "tp"),
        P(None, "tp"),
        P(None, None, "tp"),
        P(None, "tp"),
        P("tp"),
        P("tp"),
        P("tp"),
        P(None, "tp"),
        P(None, None, "tp"),
        P("ep", None, "tp"),
        P("ep", None, None, "tp"),
        P("ep", "tp", None, None),
        P("tp"),
        P("tp", None),
        P(),
        P("ep", None),
        P("ep", None),
        P("ep", None, "tp"),
        P("ep", None, "tp"),
        P("ep", "tp", None),
        P("tp", "ep"),
        P("tp", "ep"),
        P("ep", "tp"),
        P("tp"),
    )
    return jax.shard_map(
        functools.partial(local, mesh.shape["ep"], mesh.shape["tp"]),
        mesh=mesh,
        in_specs=placed,
        out_specs=(
            P("ep", "tp"),
            P("ep", "tp", None, None),
            P("ep", None, "tp"),
            P("ep", None, None, "tp"),
        ),
        check_vma=False,
    )
```

```python
import functools

import jax
import jax.numpy as jnp
from jax import lax
from jax.experimental import pallas as pl
from jax.experimental.pallas import tpu as pltpu
from jax.sharding import PartitionSpec as P

MESH = pl.DeviceIdType.MESH
F32 = jnp.float32
BF16 = jnp.bfloat16
HEAD_DIM = 64
STATE_DIM = 128
NYC = 8
UNITS = 48
eps = 1e-06


def rms_scale(values, norm_gain):
    squares = jnp.mean(values * values, axis=-1, keepdims=True)
    return values * lax.rsqrt(squares + eps) * norm_gain


def dot(a, b):
    return jnp.dot(a, b, preferred_element_type=F32)


def two_terms(v):
    high = v.astype(BF16).astype(F32)
    return high, (v - high).astype(BF16).astype(F32)


def dot_rows(a, b):
    return lax.dot_general(a, b, (((1,), (1,)), ((), ())), preferred_element_type=F32)


def layer_kernel(
    n_ep,
    n_tp,
    tokens_hbm,
    mixer_gain_hbm,
    step_weight_hbm,
    step_bias_hbm,
    decay_log_hbm,
    skip_hbm,
    inner_kernel_hbm,
    state_kernel_hbm,
    inner_window_hbm,
    state_window_hbm,
    group_gain_hbm,
    gain_hbm,
    routes_hbm,
    route_weights_hbm,
    dense_gate_hbm,
    dense_up_hbm,
    dense_down_hbm,
    dense_scale_hbm,
    gate_weight_hbm,
    inner_weight_hbm,
    state_weight_hbm,
    output_weight_hbm,
    state_hbm,
    gate_hbm,
    up_hbm,
    down_hbm,
    out_ref,
    new_inner_ref,
    new_state_window_ref,
    new_state_ref,
    gate_w,
    inner_w,
    state_w,
    output_w,
    decay_rows,
    terms,
    w_gate,
    w_up,
    w_down,
    parts,
    residual_ref,
    ffn_ref,
    dw,
    dx,
    combine_ref,
    tall,
    going,
    came,
    xs,
    act,
    dz_going,
    dz_came,
    hid,
    moe_going,
    moe_came,
    tall_back,
    back_going,
    back_came,
    od_going,
    od_came,
    tokens_ref,
    mixer_gain_ref,
    step_weight_ref,
    step_bias_ref,
    decay_log_ref,
    skip_ref,
    inner_kernel_ref,
    state_kernel_ref,
    inner_window_ref,
    state_window_ref,
    group_gain_ref,
    early_sems,
    gain_ref,
    routes_ref,
    route_weights_ref,
    dense_gate_ref,
    dense_up_ref,
    dense_down_ref,
    dense_scale_ref,
    late_sems,
    in_sems,
    state_sems,
    local_sems,
    send_sems,
    recv_sems,
):
    me = lax.axis_index("ep")
    t = lax.axis_index("tp")
    n_z = n_ep // NYC
    z = me // NYC
    yc = me % NYC
    seqs = tokens_ref.shape[0]
    heads = new_state_ref.shape[1]
    chunk = seqs // 4
    width = out_ref.shape[1]
    slots = 2 * n_ep

    def across_tp(k):
        return (me, lax.rem(t + k, n_tp))

    def along_z(k):
        return (lax.rem(z + k, n_z) * NYC + yc, t)

    def within_z(k):
        return (z * NYC + lax.rem(yc + k, NYC), t)

    def along_ep(kz, k):
        return (lax.rem(z + kz, n_z) * NYC + lax.rem(yc + k, NYC), t)

    steps = sorted(range(n_z), key=lambda kz: -min(kz, n_z - kz))

    def to_all(send, steps=steps):
        for kz in steps:
            for k in range(0 if kz else 1, NYC):
                send(kz, along_ep(kz, k))

    def remote(src, dst, which, peer):
        return pltpu.make_async_remote_copy(
            src_ref=src,
            dst_ref=dst,
            send_sem=send_sems.at[which],
            recv_sem=recv_sems.at[which],
            device_id=peer,
            device_id_type=MESH,
        )

    def wait_in(ref, which):
        remote(ref, ref, which, across_tp(1)).wait_recv()

    def wait_out(ref, which):
        remote(ref, ref, which, across_tp(1)).wait_send()

    PART, DW, DW2, DX, OUT, DZ, HID, MOE, MOE2, BACK, OD = range(11)

    early_loads = [
        pltpu.make_async_copy(src, dst, early_sems.at[i])
        for i, (src, dst) in enumerate(
            [
                (tokens_hbm, tokens_ref),
                (mixer_gain_hbm, mixer_gain_ref),
                (step_weight_hbm, step_weight_ref),
                (step_bias_hbm, step_bias_ref),
                (decay_log_hbm, decay_log_ref),
                (skip_hbm, skip_ref),
                (inner_kernel_hbm, inner_kernel_ref),
                (state_kernel_hbm, state_kernel_ref),
                (inner_window_hbm, inner_window_ref),
                (state_window_hbm, state_window_ref),
                (group_gain_hbm, group_gain_ref),
            ]
        )
    ]
    for load in early_loads:
        load.start()
    mixer_loads = [
        pltpu.make_async_copy(src, dst, in_sems.at[i])
        for i, (src, dst) in enumerate(
            [
                (inner_weight_hbm, inner_w),
                (state_weight_hbm, state_w),
                (gate_weight_hbm, gate_w),
                (output_weight_hbm, output_w),
            ]
        )
    ]
    for load in mixer_loads[:3]:
        load.start()

    barrier = pltpu.get_barrier_semaphore()
    for k in range(1, n_tp):
        pl.semaphore_signal(barrier, inc=1, device_id=across_tp(k), device_id_type=MESH)

    to_all(
        lambda kz, peer: pl.semaphore_signal(barrier, inc=1, device_id=peer, device_id_type=MESH)
    )

    state_loads = [
        pltpu.make_async_copy(
            state_hbm.at[pl.ds(c * chunk, chunk)], new_state_ref.at[pl.ds(c * chunk, chunk)], state_sems.at[c]
        )
        for c in range(4)
    ]
    for load in state_loads:
        load.start()
    mixer_loads[3].start()
    late_loads = [
        pltpu.make_async_copy(src, dst, late_sems.at[i])
        for i, (src, dst) in enumerate(
            [
                (gain_hbm, gain_ref),
                (routes_hbm, routes_ref),
                (route_weights_hbm, route_weights_ref),
                (dense_gate_hbm, dense_gate_ref),
                (dense_up_hbm, dense_up_ref),
                (dense_down_hbm, dense_down_ref),
                (dense_scale_hbm, dense_scale_ref),
            ]
        )
    ]
    for load in late_loads:
        load.start()
    for load in early_loads:
        load.wait()

    normed = rms_scale(tokens_ref[...].astype(F32), mixer_gain_ref[...]).astype(BF16)
    step_raw = dot_rows(normed, step_weight_ref[...])
    step_in = step_raw + step_bias_ref[...]
    step = jnp.maximum(step_in, 0.0) + jnp.log1p(jnp.exp(-jnp.abs(step_in)))
    decay = jnp.exp(-step * jnp.exp(decay_log_ref[...]))

    for load in mixer_loads[:3]:
        load.wait()
    inner_pre = dot(normed, inner_w[...]).astype(BF16).astype(F32)
    kern = inner_kernel_ref[...]
    conv = inner_pre * kern[3:4]
    for j in range(3):
        conv = conv + inner_window_ref[j].astype(F32) * kern[j : j + 1]
    inner = jax.nn.silu(conv)
    new_inner_ref[0:2] = inner_window_ref[1:3]
    new_inner_ref[2] = inner_pre.astype(BF16)

    vectors = []
    pres = []
    for r in range(2):
        pre = dot(normed, state_w[r]).astype(BF16).astype(F32)
        conv = pre * state_kernel_ref[3, r : r + 1, :]
        for j in range(3):
            conv = conv + state_window_ref[:, j, r, :].astype(F32) * state_kernel_ref[j, r : r + 1, :]
        vectors.append(jax.nn.silu(conv))
        pres.append(pre)
    new_state_window_ref[:, 0:2] = state_window_ref[:, 1:3]
    new_state_window_ref[:, 2] = jnp.concatenate(
        [pres[0][:, None, :], pres[1][:, None, :]], axis=1
    ).astype(BF16)
    in_vector, out_vector = vectors

    gate_pre = dot(normed, gate_w[...])

    lane = lax.broadcasted_iota(jnp.int32, inner.shape, 1) // HEAD_DIM
    step_wide = jnp.broadcast_to(step[:, 0:1], inner.shape)
    skip_wide = jnp.broadcast_to(skip_ref[:, 0:1], inner.shape)
    for h in range(1, heads):
        step_wide = jnp.where(lane == h, step[:, h : h + 1], step_wide)
        skip_wide = jnp.where(lane == h, skip_ref[:, h : h + 1], skip_wide)
    for h in range(heads):
        decay_rows[:, h * STATE_DIM : (h + 1) * STATE_DIM] = jnp.broadcast_to(
            decay[:, h : h + 1], (seqs, STATE_DIM)
        )
    spare = jnp.zeros((32 - seqs, inner.shape[1]), F32)
    high, low = two_terms(jnp.concatenate([step_wide * inner, spare], axis=0))
    written = jnp.transpose(
        jnp.concatenate([high, high, low, jnp.zeros_like(low)], axis=0)
    ).astype(BF16)
    spare = spare[:, :STATE_DIM]
    high, low = two_terms(jnp.concatenate([in_vector, spare], axis=0))
    inputs = jnp.concatenate([high, low, high, jnp.zeros_like(low)], axis=0)
    owner = lax.broadcasted_iota(jnp.int32, inputs.shape, 0) % 32
    high, low = two_terms(jnp.concatenate([out_vector, spare], axis=0))
    reader = jnp.transpose(
        jnp.concatenate([high, low, jnp.zeros((64, STATE_DIM), F32)], axis=0)
    ).astype(BF16)
    read = jnp.zeros((width, STATE_DIM), F32)
    column = lax.broadcasted_iota(jnp.int32, (heads * HEAD_DIM, STATE_DIM), 1) % 32

    for k in range(4):
        state_loads[k].wait()

        for i in range(chunk // 2):
            pair = [k * chunk + 2 * i, k * chunk + 2 * i + 1]
            added = dot(
                written,
                jnp.concatenate([jnp.where(owner == b, inputs, 0.0) for b in pair], axis=1).astype(BF16),
            )
            for n, b in enumerate(pair):
                rates = decay_rows[pl.ds(b, 1), :]
                news = []
                for h in range(heads):
                    new = new_state_ref[b, h] * rates[:, h * STATE_DIM : (h + 1) * STATE_DIM] + (
                        added[h * HEAD_DIM : (h + 1) * HEAD_DIM, n * STATE_DIM : (n + 1) * STATE_DIM]
                    )
                    new_state_ref[b, h] = new
                    news.append(new)
                at = (2 * i + n) * width
                terms[at : at + width] = jnp.concatenate(news, axis=0).astype(BF16)
        found = dot(terms[...], reader)
        for i in range(chunk):
            read = jnp.where(column == k * chunk + i, found[i * width : (i + 1) * width], read)
    mixed = jnp.transpose(read)
    mixed_rows = mixed[:seqs] + mixed[32 : 32 + seqs]
    mixed_rows = mixed_rows + skip_wide * inner
    gated = mixed_rows * jax.nn.silu(gate_pre)
    mixer_rows = (rms_scale(gated, 1.0) * group_gain_ref[...]).astype(BF16)
    mixer_loads[3].wait()
    parts[t] = dot(mixer_rows, output_w[...]).astype(BF16)

    pl.semaphore_wait(barrier, n_tp - 1 + n_ep - 1)

    for k in range(1, n_tp):
        remote(parts.at[t], parts.at[t], PART, across_tp(k)).start()

    for load in late_loads:
        load.wait()
    units = dense_gate_ref.shape[0]
    gap = jnp.zeros((UNITS - units, width), F32)
    for i, ref in enumerate((dense_gate_ref, dense_up_ref, dense_down_ref)):
        dw[yc, i * UNITS : (i + 1) * UNITS] = jnp.concatenate(
            [ref[...].astype(F32), gap], axis=0
        ).astype(BF16)

    for k in range(2, NYC, 2):
        remote(dw.at[yc], dw.at[yc], DW, within_z(k)).start()

    expert = lax.broadcasted_iota(jnp.int32, (n_ep, seqs), 0)
    named = [(routes_ref[k : k + 1, :] == expert).astype(F32) for k in range(2)]
    earlier = (
        lax.broadcasted_iota(jnp.int32, (seqs, seqs), 0)
        < lax.broadcasted_iota(jnp.int32, (seqs, seqs), 1)
    ).astype(F32)
    before = dot(named[0] + named[1], earlier)
    place = lax.broadcasted_iota(jnp.int32, (slots, seqs), 0)
    chosen = []
    for k in range(2):
        slot = jnp.sum(before * named[k], axis=0, keepdims=True).astype(jnp.int32)
        chosen.append((place == routes_ref[k : k + 1, :] * 2 + slot).astype(F32))
    selection = (chosen[0] + chosen[1]).astype(BF16)
    combine_ref[...] = jnp.transpose(
        chosen[0] * route_weights_ref[0:1, :] + chosen[1] * route_weights_ref[1:2, :]
    )

    loads = [
        pltpu.make_async_copy(src.at[0], dst, local_sems.at[i])
        for i, (src, dst) in enumerate([(gate_hbm, w_gate), (up_hbm, w_up), (down_hbm, w_down)])
    ]
    for load in loads:
        load.start()

    wait_in(parts.at[pl.ds(0, n_tp - 1)], PART)
    total = parts[0].astype(F32)
    for k in range(1, n_tp):
        total = total + parts[k].astype(F32)
    residual = tokens_ref[...].astype(F32) + total
    residual_ref[...] = residual
    ffn = rms_scale(residual, gain_ref[...]).astype(BF16)
    ffn_ref[...] = ffn

    own = pl.ds(pl.multiple_of(t * width, width), width)
    dx[z] = ffn_ref[:, own]

    for k in steps[:-1]:
        remote(dx.at[z], dx.at[z], DX, along_z(k)).start()

    outgoing = dot(selection, ffn)
    lines = outgoing.shape[1] // 128
    for j in range(lines):
        tall[pl.ds(j, slots, stride=lines), :] = outgoing[:, j * 128 : (j + 1) * 128]
    going[...] = tall[...].reshape(going.shape).astype(BF16)

    def dispatch(kz, peer):
        place = steps.index((n_z - kz) % n_z) * NYC + yc
        remote(going.at[peer[0]], came.at[place], OUT, peer).start()

    to_all(dispatch)
    came[(n_z - 1) * NYC + yc] = going[me]

    wait_in(dw.at[pl.ds(0, NYC // 2 - 1)], DW)
    sibling = (z * NYC + yc + 1 - 2 * lax.rem(yc, 2), t)
    for k in range(0, NYC, 2):
        held = lax.rem(yc + k, NYC)
        remote(dw.at[held], dw.at[held], DW2, sibling).start()
    wait_in(dw.at[pl.ds(0, NYC // 2)], DW2)
    wait_in(dx.at[pl.ds(0, n_z - 1)], DX)
    dense_rows = dx[...].reshape(n_z * seqs, width)
    for i in range(2):
        weights = dw[:, i * UNITS : (i + 1) * UNITS].reshape(NYC * UNITS, width)
        dz_going[:, :, i * NYC * UNITS : (i + 1) * NYC * UNITS] = (
            dot_rows(dense_rows, weights).astype(BF16).reshape(n_tp, -1, NYC * UNITS)
        )
    for k in range(1, n_tp):
        peer = across_tp(k)
        remote(dz_going.at[peer[1]], dz_came.at[t], DZ, peer).start()
    dz_came[t] = dz_going[t]

    wait_in(came.at[pl.ds(0, n_ep - 1)], OUT)
    wait_in(dz_came.at[pl.ds(0, n_tp - 1)], DZ)
    gate_up = dz_came[0].astype(F32)
    for k in range(1, n_tp):
        gate_up = gate_up + dz_came[k].astype(F32)
    hid[t] = (
        jax.nn.silu(gate_up[:, : NYC * UNITS]) * gate_up[:, NYC * UNITS :]
    ).astype(BF16)
    for k in range(1, n_tp):
        remote(hid.at[t], hid.at[t], HID, across_tp(k)).start()

    tall[...] = came[...].astype(F32).reshape(tall.shape)
    for j in range(lines):
        xs[:, j * 128 : (j + 1) * 128] = tall[pl.ds(j, slots, stride=lines), :].astype(BF16)
    loads[0].wait()
    loads[1].wait()
    rows = xs[...]
    act[...] = (jax.nn.silu(dot_rows(rows, w_gate[...])) * dot_rows(rows, w_up[...])).astype(BF16)
    loads[2].wait()
    halves = [pl.ds(0, n_ep), pl.ds(n_ep, n_ep)]
    for k in range(1, n_tp):
        peer = across_tp(k)
        columns = pl.ds(pl.multiple_of(peer[1] * width, width), width)
        moe_going[peer[1]] = dot(act[...], w_down[:, columns]).astype(BF16)
        half = (peer[1], halves[0])
        remote(moe_going.at[half], moe_came.at[t, halves[0]], MOE, peer).start()
    for k in range(1, n_tp):
        peer = across_tp(k)
        half = (peer[1], halves[1])
        remote(moe_going.at[half], moe_came.at[t, halves[1]], MOE2, peer).start()
    moe_came[t] = dot(act[...], w_down[:, own]).astype(BF16)

    wait_in(hid.at[pl.ds(0, n_tp - 1)], HID)
    dense_part = dot(
        hid[...].reshape(n_z * seqs, NYC * UNITS),
        dw[:, 2 * UNITS : 3 * UNITS].reshape(NYC * UNITS, width),
    )
    od_going[...] = dense_part.astype(BF16).reshape(od_going.shape)

    for k in steps[:-1]:
        there = lax.rem(z + k, n_z)
        remote(od_going.at[there], od_came.at[z], OD, along_z(k)).start()
    od_came[z] = od_going[z]

    for n, which in enumerate((MOE, MOE2)):
        wait_in(moe_came.at[pl.ds(0, n_tp - 1), halves[n]], which)
        rows_out = moe_came[0, halves[n]].astype(F32)
        for k in range(1, n_tp):
            rows_out = rows_out + moe_came[k, halves[n]].astype(F32)
        lines = pl.ds(n * slots, slots)
        for j in range(width // 128):
            tall_back[pl.ds(n * slots + j, n_ep, stride=2), :] = rows_out[:, j * 128 : (j + 1) * 128]
        back_going[pl.ds(n * n_ep // 2, n_ep // 2)] = (
            tall_back[lines].reshape(n_ep // 2, 4, 128).astype(BF16)
        )

        def give_back(kz, peer):
            place = steps.index(kz) * NYC + peer[0] % NYC
            remote(back_going.at[place], back_came.at[me], BACK, peer).start()

        to_all(give_back, steps[n * n_z // 2 : (n + 1) * n_z // 2])
    back_came[me] = back_going[(n_z - 1) * NYC + yc]

    wait_in(od_came.at[pl.ds(0, n_z - 1)], OD)
    dense_out = od_came[0].astype(F32)
    for k in range(1, n_z):
        dense_out = dense_out + od_came[k].astype(F32)

    wait_in(back_came.at[pl.ds(0, n_ep - 1)], BACK)
    tall_back[...] = back_came[...].astype(F32).reshape(tall_back.shape)
    returned = [
        tall_back[pl.ds(j, slots, stride=2), :].astype(BF16) for j in range(width // 128)
    ]
    returned = jnp.concatenate(returned, axis=1).astype(F32)
    expert_out = jnp.dot(combine_ref[...], returned, precision=lax.Precision.HIGHEST)
    out_ref[...] = (
        residual_ref[:, own] + expert_out + dense_scale_ref[...] * dense_out
    ).astype(BF16)

    wait_out(parts.at[pl.ds(0, n_tp - 1)], PART)
    wait_out(dw.at[pl.ds(0, NYC // 2 - 1)], DW)
    wait_out(dw.at[pl.ds(0, NYC // 2)], DW2)
    wait_out(dx.at[pl.ds(0, n_z - 1)], DX)
    wait_out(going.at[pl.ds(0, n_ep - 1)], OUT)
    wait_out(dz_going.at[pl.ds(0, n_tp - 1)], DZ)
    wait_out(hid.at[pl.ds(0, n_tp - 1)], HID)
    wait_out(moe_going.at[pl.ds(0, n_tp - 1), halves[0]], MOE)
    wait_out(moe_going.at[pl.ds(0, n_tp - 1), halves[1]], MOE2)
    wait_out(back_going.at[pl.ds(0, n_ep - 1)], BACK)
    wait_out(od_going.at[pl.ds(0, n_z - 1)], OD)


def write_kernel(*refs):
    sems = refs[-1]
    copies = [pltpu.make_async_copy(refs[i], refs[4 + i], sems.at[i]) for i in (3, 0, 1, 2)]
    for copy in copies:
        copy.start()
    for copy in copies:
        copy.wait()


VMEM = pl.BlockSpec(memory_space=pltpu.VMEM)
ANY = pl.BlockSpec(memory_space=pl.ANY)


def local(
    n_ep,
    n_tp,
    tokens,
    mixer_gain,
    gate_weight,
    inner_weight,
    state_weight,
    step_weight,
    step_bias,
    decay_log,
    skip_scale,
    inner_kernel,
    state_kernel,
    inner_window,
    state_window,
    recurrent_state,
    group_gain,
    output_weight,
    channel_gain,
    routes,
    route_weights,
    expert_gate,
    expert_up,
    expert_down,
    dense_gate,
    dense_up,
    dense_down,
    dense_scale,
):
    seqs, model = tokens.shape
    width = dense_scale.shape[0]
    hidden = expert_gate.shape[2]
    n_z = n_ep // NYC
    slots = 2 * n_ep
    early = (
        tokens,
        mixer_gain[None],
        step_weight.T,
        step_bias[None],
        decay_log[None],
        skip_scale[None],
        inner_kernel,
        state_kernel,
        jnp.swapaxes(inner_window, 0, 1),
        state_window,
        group_gain[None],
    )
    late = (
        channel_gain[None],
        routes.T,
        route_weights.T,
        dense_gate.T,
        dense_up.T,
        dense_down,
        dense_scale[None],
    )
    scratch = [
        pltpu.VMEM(gate_weight.shape, BF16),
        pltpu.VMEM(inner_weight.shape, BF16),
        pltpu.VMEM(state_weight.shape, BF16),
        pltpu.VMEM(output_weight.shape, BF16),
        pltpu.VMEM((seqs, step_bias.shape[0] * STATE_DIM), F32),
        pltpu.VMEM((seqs // 4 * width, STATE_DIM), BF16),
        pltpu.VMEM((hidden, model), BF16),
        pltpu.VMEM((hidden, model), BF16),
        pltpu.VMEM((hidden, model), BF16),
        pltpu.VMEM((n_tp, seqs, model), BF16),
        pltpu.VMEM((seqs, model), F32),
        pltpu.VMEM((seqs, model), BF16),
        pltpu.VMEM((NYC, 3 * UNITS, width), BF16),
        pltpu.VMEM((n_z, seqs, width), BF16),
        pltpu.VMEM((seqs, slots), F32),
        pltpu.VMEM((slots * model // 128, 128), F32),
        pltpu.VMEM((n_ep, 2 * model // 128, 128), BF16),
        pltpu.VMEM((n_ep, 2 * model // 128, 128), BF16),
        pltpu.VMEM((slots, model), BF16),
        pltpu.VMEM((slots, hidden), BF16),
        pltpu.VMEM((n_tp, n_z * seqs // n_tp, 2 * NYC * UNITS), BF16),
        pltpu.VMEM((n_tp, n_z * seqs // n_tp, 2 * NYC * UNITS), BF16),
        pltpu.VMEM((n_tp, n_z * seqs // n_tp, NYC * UNITS), BF16),
        pltpu.VMEM((n_tp, slots, width), BF16),
        pltpu.VMEM((n_tp, slots, width), BF16),
        pltpu.VMEM((slots * 2, 128), F32),
        pltpu.VMEM((n_ep, 4, 128), BF16),
        pltpu.VMEM((n_ep, 4, 128), BF16),
        pltpu.VMEM((n_z, seqs, width), BF16),
        pltpu.VMEM((n_z, seqs, width), BF16),
        *[pltpu.VMEM(x.shape, x.dtype) for x in early],
        pltpu.SemaphoreType.DMA((len(early),)),
        *[pltpu.VMEM(x.shape, x.dtype) for x in late],
        pltpu.SemaphoreType.DMA((len(late),)),
        pltpu.SemaphoreType.DMA((4,)),
        pltpu.SemaphoreType.DMA((4,)),
        pltpu.SemaphoreType.DMA((3,)),
        pltpu.SemaphoreType.DMA((11,)),
        pltpu.SemaphoreType.DMA((11,)),
    ]
    results = [
        ((seqs, width), BF16),
        ((3, seqs, width), BF16),
        (state_window.shape, BF16),
        (recurrent_state.shape, F32),
    ]
    held = pl.pallas_call(
        functools.partial(layer_kernel, n_ep, n_tp),
        out_shape=tuple(pltpu.VMEM(*r) for r in results),
        in_specs=[ANY] * 26,
        out_specs=(VMEM,) * 4,
        scratch_shapes=scratch,
        compiler_params=pltpu.CompilerParams(collective_id=0, has_side_effects=True),
        name="layer",
    )(
        *early,
        *late,
        gate_weight,
        inner_weight,
        state_weight,
        output_weight,
        recurrent_state,
        jnp.swapaxes(expert_gate, 1, 2),
        jnp.swapaxes(expert_up, 1, 2),
        expert_down,
    )
    new_tokens, new_inner, new_window, new_state = pl.pallas_call(
        write_kernel,
        out_shape=tuple(jax.ShapeDtypeStruct(*r) for r in results),
        in_specs=[VMEM] * 4,
        out_specs=(ANY,) * 4,
        scratch_shapes=[pltpu.SemaphoreType.DMA((4,))],
        name="write",
    )(*(pltpu.with_memory_space_constraint(h, pltpu.VMEM) for h in held))
    return new_tokens, new_state, jnp.swapaxes(new_inner, 0, 1), new_window


def solution(mesh):
    placed = (
        P("ep", None),
        P(),
        P(None, "tp"),
        P(None, "tp"),
        P(None, None, "tp"),
        P(None, "tp"),
        P("tp"),
        P("tp"),
        P("tp"),
        P(None, "tp"),
        P(None, None, "tp"),
        P("ep", None, "tp"),
        P("ep", None, None, "tp"),
        P("ep", "tp", None, None),
        P("tp"),
        P("tp", None),
        P(),
        P("ep", None),
        P("ep", None),
        P("ep", None, "tp"),
        P("ep", None, "tp"),
        P("ep", "tp", None),
        P("tp", "ep"),
        P("tp", "ep"),
        P("ep", "tp"),
        P("tp"),
    )
    return jax.shard_map(
        functools.partial(local, mesh.shape["ep"], mesh.shape["tp"]),
        mesh=mesh,
        in_specs=placed,
        out_specs=(
            P("ep", "tp"),
            P("ep", "tp", None, None),
            P("ep", None, "tp"),
            P("ep", None, None, "tp"),
        ),
        check_vma=False,
    )
```

```python
import functools

import jax
import jax.numpy as jnp
from jax import lax
from jax.experimental import pallas as pl
from jax.experimental.pallas import tpu as pltpu
from jax.sharding import PartitionSpec as P

MESH = pl.DeviceIdType.MESH
F32 = jnp.float32
BF16 = jnp.bfloat16
HEAD_DIM = 64
STATE_DIM = 128
NYC = 8
UNITS = 48
eps = 1e-06


def rms_scale(values, norm_gain):
    squares = jnp.mean(values * values, axis=-1, keepdims=True)
    return values * lax.rsqrt(squares + eps) * norm_gain


def dot(a, b):
    return jnp.dot(a, b, preferred_element_type=F32)


def two_terms(v):
    high = v.astype(BF16).astype(F32)
    return high, (v - high).astype(BF16).astype(F32)


def dot_rows(a, b):
    return lax.dot_general(a, b, (((1,), (1,)), ((), ())), preferred_element_type=F32)


def layer_kernel(
    n_ep,
    n_tp,
    tokens_hbm,
    mixer_gain_hbm,
    step_weight_hbm,
    step_bias_hbm,
    decay_log_hbm,
    skip_hbm,
    inner_kernel_hbm,
    state_kernel_hbm,
    inner_window_hbm,
    state_window_hbm,
    group_gain_hbm,
    gain_hbm,
    routes_hbm,
    route_weights_hbm,
    dense_gate_hbm,
    dense_up_hbm,
    dense_down_hbm,
    dense_scale_hbm,
    gate_weight_hbm,
    inner_weight_hbm,
    state_weight_hbm,
    output_weight_hbm,
    state_hbm,
    gate_hbm,
    up_hbm,
    down_hbm,
    out_ref,
    new_inner_ref,
    new_state_window_ref,
    new_state_ref,
    gate_w,
    inner_w,
    state_w,
    output_w,
    decay_rows,
    w_gate,
    w_up,
    w_down,
    parts,
    residual_ref,
    ffn_ref,
    dw,
    dx,
    combine_ref,
    tall,
    going,
    came,
    xs,
    act,
    dz_going,
    dz_came,
    hid,
    moe_going,
    moe_came,
    tall_back,
    back_going,
    back_came,
    od_going,
    od_came,
    tokens_ref,
    mixer_gain_ref,
    step_weight_ref,
    step_bias_ref,
    decay_log_ref,
    skip_ref,
    inner_kernel_ref,
    state_kernel_ref,
    inner_window_ref,
    state_window_ref,
    group_gain_ref,
    early_sems,
    gain_ref,
    routes_ref,
    route_weights_ref,
    dense_gate_ref,
    dense_up_ref,
    dense_down_ref,
    dense_scale_ref,
    late_sems,
    in_sems,
    state_sems,
    local_sems,
    send_sems,
    recv_sems,
    rounds,
):
    me = lax.axis_index("ep")
    t = lax.axis_index("tp")
    n_z = n_ep // NYC
    z = me // NYC
    yc = me % NYC
    seqs = tokens_ref.shape[0]
    heads = new_state_ref.shape[1]
    chunk = seqs // 4
    width = out_ref.shape[1]
    slots = 2 * n_ep

    def across_tp(k):
        return (me, lax.rem(t + k, n_tp))

    def along_z(k):
        return (lax.rem(z + k, n_z) * NYC + yc, t)

    def within_z(k):
        return (z * NYC + lax.rem(yc + k, NYC), t)

    def along_ep(kz, k):
        return (lax.rem(z + kz, n_z) * NYC + lax.rem(yc + k, NYC), t)

    steps = sorted(range(n_z), key=lambda kz: -min(kz, n_z - kz))

    def to_all(send, steps=steps):
        for kz in steps:
            for k in range(0 if kz else 1, NYC):
                send(kz, along_ep(kz, k))

    def remote(src, dst, which, peer):
        return pltpu.make_async_remote_copy(
            src_ref=src,
            dst_ref=dst,
            send_sem=send_sems.at[which],
            recv_sem=recv_sems.at[which],
            device_id=peer,
            device_id_type=MESH,
        )

    def wait_in(ref, which):
        remote(ref, ref, which, across_tp(1)).wait_recv()

    def wait_out(ref, which):
        remote(ref, ref, which, across_tp(1)).wait_send()

    PART, DW, DW2, DX, OUT, DZ, HID, MOE, MOE2, BACK, OD = range(11)

    early_loads = [
        pltpu.make_async_copy(src, dst, early_sems.at[i])
        for i, (src, dst) in enumerate(
            [
                (tokens_hbm, tokens_ref),
                (mixer_gain_hbm, mixer_gain_ref),
                (step_weight_hbm, step_weight_ref),
                (step_bias_hbm, step_bias_ref),
                (decay_log_hbm, decay_log_ref),
                (skip_hbm, skip_ref),
                (inner_kernel_hbm, inner_kernel_ref),
                (state_kernel_hbm, state_kernel_ref),
                (inner_window_hbm, inner_window_ref),
                (state_window_hbm, state_window_ref),
                (group_gain_hbm, group_gain_ref),
            ]
        )
    ]
    for load in early_loads:
        load.start()
    mixer_loads = [
        pltpu.make_async_copy(src, dst, in_sems.at[i])
        for i, (src, dst) in enumerate(
            [
                (inner_weight_hbm, inner_w),
                (state_weight_hbm, state_w),
                (gate_weight_hbm, gate_w),
                (output_weight_hbm, output_w),
            ]
        )
    ]
    for load in mixer_loads[:3]:
        load.start()

    barrier = pltpu.get_barrier_semaphore()
    for k in range(1, n_tp):
        pl.semaphore_signal(barrier, inc=1, device_id=across_tp(k), device_id_type=MESH)

    for k in range(1, NYC):
        pl.semaphore_signal(barrier, inc=1, device_id=within_z(k), device_id_type=MESH)
    for k in (1, n_z - 1):
        pl.semaphore_signal(barrier, inc=1, device_id=along_z(k), device_id_type=MESH)

    state_loads = [
        pltpu.make_async_copy(
            state_hbm.at[pl.ds(c * chunk, chunk)], new_state_ref.at[pl.ds(c * chunk, chunk)], state_sems.at[c]
        )
        for c in range(4)
    ]
    for load in state_loads:
        load.start()
    mixer_loads[3].start()
    late_loads = [
        pltpu.make_async_copy(src, dst, late_sems.at[i])
        for i, (src, dst) in enumerate(
            [
                (gain_hbm, gain_ref),
                (routes_hbm, routes_ref),
                (route_weights_hbm, route_weights_ref),
                (dense_gate_hbm, dense_gate_ref),
                (dense_up_hbm, dense_up_ref),
                (dense_down_hbm, dense_down_ref),
                (dense_scale_hbm, dense_scale_ref),
            ]
        )
    ]
    for load in late_loads:
        load.start()
    for load in early_loads:
        load.wait()

    normed = rms_scale(tokens_ref[...].astype(F32), mixer_gain_ref[...]).astype(BF16)
    step_raw = dot_rows(normed, step_weight_ref[...])
    step_in = step_raw + step_bias_ref[...]
    step = jnp.maximum(step_in, 0.0) + jnp.log1p(jnp.exp(-jnp.abs(step_in)))
    decay = jnp.exp(-step * jnp.exp(decay_log_ref[...]))

    for load in mixer_loads[:3]:
        load.wait()
    inner_pre = dot(normed, inner_w[...]).astype(BF16).astype(F32)
    kern = inner_kernel_ref[...]
    conv = inner_pre * kern[3:4]
    for j in range(3):
        conv = conv + inner_window_ref[j].astype(F32) * kern[j : j + 1]
    inner = jax.nn.silu(conv)
    new_inner_ref[0:2] = inner_window_ref[1:3]
    new_inner_ref[2] = inner_pre.astype(BF16)

    vectors = []
    pres = []
    for r in range(2):
        pre = dot(normed, state_w[r]).astype(BF16).astype(F32)
        conv = pre * state_kernel_ref[3, r : r + 1, :]
        for j in range(3):
            conv = conv + state_window_ref[:, j, r, :].astype(F32) * state_kernel_ref[j, r : r + 1, :]
        vectors.append(jax.nn.silu(conv))
        pres.append(pre)
    new_state_window_ref[:, 0:2] = state_window_ref[:, 1:3]
    new_state_window_ref[:, 2] = jnp.concatenate(
        [pres[0][:, None, :], pres[1][:, None, :]], axis=1
    ).astype(BF16)
    in_vector, out_vector = vectors

    gate_pre = dot(normed, gate_w[...])

    lane = lax.broadcasted_iota(jnp.int32, inner.shape, 1) // HEAD_DIM

    def widen(v):
        wide = jnp.broadcast_to(v[:, 0:1], inner.shape)
        for h in range(1, heads):
            wide = jnp.where(lane == h, v[:, h : h + 1], wide)
        return wide

    spare = jnp.zeros((32 - seqs, STATE_DIM), F32)
    high, low = two_terms(jnp.concatenate([out_vector, spare], axis=0))
    reader = jnp.transpose(
        jnp.concatenate([high, low, jnp.zeros((64, STATE_DIM), F32)], axis=0)
    ).astype(BF16)
    read = jnp.zeros((width, STATE_DIM), F32)
    column = lax.broadcasted_iota(jnp.int32, (width, STATE_DIM), 1) % 32
    written_rows = widen(step) * inner
    fresh = written_rows * jnp.sum(in_vector * out_vector, axis=1, keepdims=True)
    fresh = fresh + widen(skip_ref[...]) * inner
    decay_wide = widen(decay)
    opened = jax.nn.silu(gate_pre)

    pl.semaphore_wait(barrier, n_tp - 1 + NYC - 1 + 2)
    for k in (1, n_z - 1):
        pl.semaphore_signal(rounds.at[0], inc=1, device_id=along_z(k), device_id_type=MESH)

    for k in range(4):
        state_loads[k].wait()
        olds = new_state_ref[k * chunk : (k + 1) * chunk].reshape(chunk * width, STATE_DIM)
        found = dot(olds.astype(BF16), reader)
        for i in range(chunk):
            read = jnp.where(column == k * chunk + i, found[i * width : (i + 1) * width], read)
    pl.semaphore_wait(rounds.at[0], 2)
    for k in (2, n_z - 2):
        pl.semaphore_signal(rounds.at[1], inc=1, device_id=along_z(k), device_id_type=MESH)

    mixed = jnp.transpose(read)
    gated = (decay_wide * (mixed[:seqs] + mixed[32 : 32 + seqs]) + fresh) * opened
    mixer_rows = (rms_scale(gated, 1.0) * group_gain_ref[...]).astype(BF16)
    mixer_loads[3].wait()
    parts[t] = dot(mixer_rows, output_w[...]).astype(BF16)

    for k in range(1, n_tp):
        remote(parts.at[t], parts.at[t], PART, across_tp(k)).start()

    for load in late_loads:
        load.wait()
    units = dense_gate_ref.shape[0]
    gap = jnp.zeros((UNITS - units, width), F32)
    for i, ref in enumerate((dense_gate_ref, dense_up_ref, dense_down_ref)):
        dw[yc, i * UNITS : (i + 1) * UNITS] = jnp.concatenate(
            [ref[...].astype(F32), gap], axis=0
        ).astype(BF16)

    for k in range(2, NYC, 2):
        remote(dw.at[yc], dw.at[yc], DW, within_z(k)).start()

    expert = lax.broadcasted_iota(jnp.int32, (n_ep, seqs), 0)
    named = [(routes_ref[k : k + 1, :] == expert).astype(F32) for k in range(2)]
    earlier = (
        lax.broadcasted_iota(jnp.int32, (seqs, seqs), 0)
        < lax.broadcasted_iota(jnp.int32, (seqs, seqs), 1)
    ).astype(F32)
    before = dot(named[0] + named[1], earlier)
    place = lax.broadcasted_iota(jnp.int32, (slots, seqs), 0)
    chosen = []
    for k in range(2):
        slot = jnp.sum(before * named[k], axis=0, keepdims=True).astype(jnp.int32)
        chosen.append((place == routes_ref[k : k + 1, :] * 2 + slot).astype(F32))
    selection = (chosen[0] + chosen[1]).astype(BF16)
    combine_ref[...] = jnp.transpose(
        chosen[0] * route_weights_ref[0:1, :] + chosen[1] * route_weights_ref[1:2, :]
    )

    loads = [
        pltpu.make_async_copy(src.at[0], dst, local_sems.at[i])
        for i, (src, dst) in enumerate([(gate_hbm, w_gate), (up_hbm, w_up), (down_hbm, w_down)])
    ]
    for load in loads:
        load.start()

    pl.semaphore_wait(rounds.at[1], 2)
    for k in range(1, NYC):
        pl.semaphore_signal(rounds.at[2], inc=1, device_id=within_z(k), device_id_type=MESH)

    for h in range(heads):
        decay_rows[:, h * STATE_DIM : (h + 1) * STATE_DIM] = jnp.broadcast_to(
            decay[:, h : h + 1], (seqs, STATE_DIM)
        )
    high, low = two_terms(
        jnp.concatenate([written_rows, jnp.zeros((32 - seqs, width), F32)], axis=0)
    )
    written = jnp.transpose(
        jnp.concatenate([high, high, low, jnp.zeros_like(low)], axis=0)
    ).astype(BF16)
    high, low = two_terms(jnp.concatenate([in_vector, spare], axis=0))
    inputs = jnp.concatenate([high, low, high, jnp.zeros_like(low)], axis=0)
    owner = lax.broadcasted_iota(jnp.int32, inputs.shape, 0) % 32
    for first in range(0, seqs, 2):
        pair = (first, first + 1)
        added = dot(
            written,
            jnp.concatenate([jnp.where(owner == b, inputs, 0.0) for b in pair], axis=1).astype(BF16),
        )
        for n, b in enumerate(pair):
            rates = decay_rows[b : b + 1, :]
            for h in range(heads):
                new_state_ref[b, h] = new_state_ref[b, h] * rates[:, h * STATE_DIM : (h + 1) * STATE_DIM] + (
                    added[h * HEAD_DIM : (h + 1) * HEAD_DIM, n * STATE_DIM : (n + 1) * STATE_DIM]
                )

    wait_in(parts.at[pl.ds(0, n_tp - 1)], PART)
    total = parts[0].astype(F32)
    for k in range(1, n_tp):
        total = total + parts[k].astype(F32)
    residual = tokens_ref[...].astype(F32) + total
    residual_ref[...] = residual
    ffn = rms_scale(residual, gain_ref[...]).astype(BF16)
    ffn_ref[...] = ffn

    own = pl.ds(pl.multiple_of(t * width, width), width)
    dx[z] = ffn_ref[:, own]

    for k in steps[:-1]:
        remote(dx.at[z], dx.at[z], DX, along_z(k)).start()

    outgoing = dot(selection, ffn)
    lines = outgoing.shape[1] // 128
    for j in range(lines):
        tall[pl.ds(j, slots, stride=lines), :] = outgoing[:, j * 128 : (j + 1) * 128]
    going[...] = tall[...].reshape(going.shape).astype(BF16)

    pl.semaphore_wait(rounds.at[2], NYC - 1)
    def dispatch(kz, peer):
        place = steps.index((n_z - kz) % n_z) * NYC + yc
        remote(going.at[peer[0]], came.at[place], OUT, peer).start()

    to_all(dispatch)
    came[(n_z - 1) * NYC + yc] = going[me]

    wait_in(dw.at[pl.ds(0, NYC // 2 - 1)], DW)
    sibling = (z * NYC + yc + 1 - 2 * lax.rem(yc, 2), t)
    for k in range(0, NYC, 2):
        held = lax.rem(yc + k, NYC)
        remote(dw.at[held], dw.at[held], DW2, sibling).start()
    wait_in(dw.at[pl.ds(0, NYC // 2)], DW2)
    wait_in(dx.at[pl.ds(0, n_z - 1)], DX)
    dense_rows = dx[...].reshape(n_z * seqs, width)
    for i in range(2):
        weights = dw[:, i * UNITS : (i + 1) * UNITS].reshape(NYC * UNITS, width)
        dz_going[:, :, i * NYC * UNITS : (i + 1) * NYC * UNITS] = (
            dot_rows(dense_rows, weights).astype(BF16).reshape(n_tp, -1, NYC * UNITS)
        )
    for k in range(1, n_tp):
        peer = across_tp(k)
        remote(dz_going.at[peer[1]], dz_came.at[t], DZ, peer).start()
    dz_came[t] = dz_going[t]

    wait_in(came.at[pl.ds(0, n_ep - 1)], OUT)
    tall[...] = came[...].astype(F32).reshape(tall.shape)
    for j in range(lines):
        xs[:, j * 128 : (j + 1) * 128] = tall[pl.ds(j, slots, stride=lines), :].astype(BF16)
    loads[0].wait()
    loads[1].wait()
    rows = xs[...]
    act[...] = (jax.nn.silu(dot_rows(rows, w_gate[...])) * dot_rows(rows, w_up[...])).astype(BF16)
    loads[2].wait()
    halves = [pl.ds(0, n_ep), pl.ds(n_ep, n_ep)]
    for k in range(1, n_tp):
        peer = across_tp(k)
        columns = pl.ds(pl.multiple_of(peer[1] * width, width), width)
        moe_going[peer[1]] = dot(act[...], w_down[:, columns]).astype(BF16)
        half = (peer[1], halves[0])
        remote(moe_going.at[half], moe_came.at[t, halves[0]], MOE, peer).start()
    for k in range(1, n_tp):
        peer = across_tp(k)
        half = (peer[1], halves[1])
        remote(moe_going.at[half], moe_came.at[t, halves[1]], MOE2, peer).start()
    moe_came[t] = dot(act[...], w_down[:, own]).astype(BF16)

    wait_in(dz_came.at[pl.ds(0, n_tp - 1)], DZ)
    gate_up = dz_came[0].astype(F32)
    for k in range(1, n_tp):
        gate_up = gate_up + dz_came[k].astype(F32)
    hid[t] = (
        jax.nn.silu(gate_up[:, : NYC * UNITS]) * gate_up[:, NYC * UNITS :]
    ).astype(BF16)
    for k in range(1, n_tp):
        remote(hid.at[t], hid.at[t], HID, across_tp(k)).start()

    for n, which in enumerate((MOE, MOE2)):
        wait_in(moe_came.at[pl.ds(0, n_tp - 1), halves[n]], which)
        rows_out = moe_came[0, halves[n]].astype(F32)
        for k in range(1, n_tp):
            rows_out = rows_out + moe_came[k, halves[n]].astype(F32)
        lines = pl.ds(n * slots, slots)
        for j in range(width // 128):
            tall_back[pl.ds(n * slots + j, n_ep, stride=2), :] = rows_out[:, j * 128 : (j + 1) * 128]
        back_going[pl.ds(n * n_ep // 2, n_ep // 2)] = (
            tall_back[lines].reshape(n_ep // 2, 4, 128).astype(BF16)
        )

        def give_back(kz, peer):
            place = steps.index(kz) * NYC + peer[0] % NYC
            remote(back_going.at[place], back_came.at[me], BACK, peer).start()

        to_all(give_back, steps[n * n_z // 2 : (n + 1) * n_z // 2])
    back_came[me] = back_going[(n_z - 1) * NYC + yc]

    wait_in(hid.at[pl.ds(0, n_tp - 1)], HID)
    dense_part = dot(
        hid[...].reshape(n_z * seqs, NYC * UNITS),
        dw[:, 2 * UNITS : 3 * UNITS].reshape(NYC * UNITS, width),
    )
    od_going[...] = dense_part.astype(BF16).reshape(od_going.shape)

    for k in steps[:-1]:
        there = lax.rem(z + k, n_z)
        remote(od_going.at[there], od_came.at[z], OD, along_z(k)).start()
    od_came[z] = od_going[z]

    wait_in(od_came.at[pl.ds(0, n_z - 1)], OD)
    dense_out = od_came[0].astype(F32)
    for k in range(1, n_z):
        dense_out = dense_out + od_came[k].astype(F32)

    wait_in(back_came.at[pl.ds(0, n_ep - 1)], BACK)
    tall_back[...] = back_came[...].astype(F32).reshape(tall_back.shape)
    returned = [
        tall_back[pl.ds(j, slots, stride=2), :].astype(BF16) for j in range(width // 128)
    ]
    returned = jnp.concatenate(returned, axis=1).astype(F32)
    expert_out = jnp.dot(combine_ref[...], returned, precision=lax.Precision.HIGHEST)
    out_ref[...] = (
        residual_ref[:, own] + expert_out + dense_scale_ref[...] * dense_out
    ).astype(BF16)

    wait_out(parts.at[pl.ds(0, n_tp - 1)], PART)
    wait_out(dw.at[pl.ds(0, NYC // 2 - 1)], DW)
    wait_out(dw.at[pl.ds(0, NYC // 2)], DW2)
    wait_out(dx.at[pl.ds(0, n_z - 1)], DX)
    wait_out(going.at[pl.ds(0, n_ep - 1)], OUT)
    wait_out(dz_going.at[pl.ds(0, n_tp - 1)], DZ)
    wait_out(hid.at[pl.ds(0, n_tp - 1)], HID)
    wait_out(moe_going.at[pl.ds(0, n_tp - 1), halves[0]], MOE)
    wait_out(moe_going.at[pl.ds(0, n_tp - 1), halves[1]], MOE2)
    wait_out(back_going.at[pl.ds(0, n_ep - 1)], BACK)
    wait_out(od_going.at[pl.ds(0, n_z - 1)], OD)


def write_kernel(*refs):
    sems = refs[-1]
    copies = [pltpu.make_async_copy(refs[i], refs[4 + i], sems.at[i]) for i in (3, 0, 1, 2)]
    for copy in copies:
        copy.start()
    for copy in copies:
        copy.wait()


VMEM = pl.BlockSpec(memory_space=pltpu.VMEM)
ANY = pl.BlockSpec(memory_space=pl.ANY)


def local(
    n_ep,
    n_tp,
    tokens,
    mixer_gain,
    gate_weight,
    inner_weight,
    state_weight,
    step_weight,
    step_bias,
    decay_log,
    skip_scale,
    inner_kernel,
    state_kernel,
    inner_window,
    state_window,
    recurrent_state,
    group_gain,
    output_weight,
    channel_gain,
    routes,
    route_weights,
    expert_gate,
    expert_up,
    expert_down,
    dense_gate,
    dense_up,
    dense_down,
    dense_scale,
):
    seqs, model = tokens.shape
    width = dense_scale.shape[0]
    hidden = expert_gate.shape[2]
    n_z = n_ep // NYC
    slots = 2 * n_ep
    early = (
        tokens,
        mixer_gain[None],
        step_weight.T,
        step_bias[None],
        decay_log[None],
        skip_scale[None],
        inner_kernel,
        state_kernel,
        jnp.swapaxes(inner_window, 0, 1),
        state_window,
        group_gain[None],
    )
    late = (
        channel_gain[None],
        routes.T,
        route_weights.T,
        dense_gate.T,
        dense_up.T,
        dense_down,
        dense_scale[None],
    )
    scratch = [
        pltpu.VMEM(gate_weight.shape, BF16),
        pltpu.VMEM(inner_weight.shape, BF16),
        pltpu.VMEM(state_weight.shape, BF16),
        pltpu.VMEM(output_weight.shape, BF16),
        pltpu.VMEM((seqs, step_bias.shape[0] * STATE_DIM), F32),
        pltpu.VMEM((hidden, model), BF16),
        pltpu.VMEM((hidden, model), BF16),
        pltpu.VMEM((hidden, model), BF16),
        pltpu.VMEM((n_tp, seqs, model), BF16),
        pltpu.VMEM((seqs, model), F32),
        pltpu.VMEM((seqs, model), BF16),
        pltpu.VMEM((NYC, 3 * UNITS, width), BF16),
        pltpu.VMEM((n_z, seqs, width), BF16),
        pltpu.VMEM((seqs, slots), F32),
        pltpu.VMEM((slots * model // 128, 128), F32),
        pltpu.VMEM((n_ep, 2 * model // 128, 128), BF16),
        pltpu.VMEM((n_ep, 2 * model // 128, 128), BF16),
        pltpu.VMEM((slots, model), BF16),
        pltpu.VMEM((slots, hidden), BF16),
        pltpu.VMEM((n_tp, n_z * seqs // n_tp, 2 * NYC * UNITS), BF16),
        pltpu.VMEM((n_tp, n_z * seqs // n_tp, 2 * NYC * UNITS), BF16),
        pltpu.VMEM((n_tp, n_z * seqs // n_tp, NYC * UNITS), BF16),
        pltpu.VMEM((n_tp, slots, width), BF16),
        pltpu.VMEM((n_tp, slots, width), BF16),
        pltpu.VMEM((slots * 2, 128), F32),
        pltpu.VMEM((n_ep, 4, 128), BF16),
        pltpu.VMEM((n_ep, 4, 128), BF16),
        pltpu.VMEM((n_z, seqs, width), BF16),
        pltpu.VMEM((n_z, seqs, width), BF16),
        *[pltpu.VMEM(x.shape, x.dtype) for x in early],
        pltpu.SemaphoreType.DMA((len(early),)),
        *[pltpu.VMEM(x.shape, x.dtype) for x in late],
        pltpu.SemaphoreType.DMA((len(late),)),
        pltpu.SemaphoreType.DMA((4,)),
        pltpu.SemaphoreType.DMA((4,)),
        pltpu.SemaphoreType.DMA((3,)),
        pltpu.SemaphoreType.DMA((11,)),
        pltpu.SemaphoreType.DMA((11,)),
        pltpu.SemaphoreType.REGULAR((3,)),
    ]
    results = [
        ((seqs, width), BF16),
        ((3, seqs, width), BF16),
        (state_window.shape, BF16),
        (recurrent_state.shape, F32),
    ]
    held = pl.pallas_call(
        functools.partial(layer_kernel, n_ep, n_tp),
        out_shape=tuple(pltpu.VMEM(*r) for r in results),
        in_specs=[ANY] * 26,
        out_specs=(VMEM,) * 4,
        scratch_shapes=scratch,
        compiler_params=pltpu.CompilerParams(collective_id=0, has_side_effects=True),
        name="layer",
    )(
        *early,
        *late,
        gate_weight,
        inner_weight,
        state_weight,
        output_weight,
        recurrent_state,
        jnp.swapaxes(expert_gate, 1, 2),
        jnp.swapaxes(expert_up, 1, 2),
        expert_down,
    )
    new_tokens, new_inner, new_window, new_state = pl.pallas_call(
        write_kernel,
        out_shape=tuple(jax.ShapeDtypeStruct(*r) for r in results),
        in_specs=[VMEM] * 4,
        out_specs=(ANY,) * 4,
        scratch_shapes=[pltpu.SemaphoreType.DMA((4,))],
        name="write",
    )(*(pltpu.with_memory_space_constraint(h, pltpu.VMEM) for h in held))
    return new_tokens, new_state, jnp.swapaxes(new_inner, 0, 1), new_window


def solution(mesh):
    placed = (
        P("ep", None),
        P(),
        P(None, "tp"),
        P(None, "tp"),
        P(None, None, "tp"),
        P(None, "tp"),
        P("tp"),
        P("tp"),
        P("tp"),
        P(None, "tp"),
        P(None, None, "tp"),
        P("ep", None, "tp"),
        P("ep", None, None, "tp"),
        P("ep", "tp", None, None),
        P("tp"),
        P("tp", None),
        P(),
        P("ep", None),
        P("ep", None),
        P("ep", None, "tp"),
        P("ep", None, "tp"),
        P("ep", "tp", None),
        P("tp", "ep"),
        P("tp", "ep"),
        P("ep", "tp"),
        P("tp"),
    )
    return jax.shard_map(
        functools.partial(local, mesh.shape["ep"], mesh.shape["tp"]),
        mesh=mesh,
        in_specs=placed,
        out_specs=(
            P("ep", "tp"),
            P("ep", "tp", None, None),
            P("ep", None, "tp"),
            P("ep", None, None, "tp"),
        ),
        check_vma=False,
    )
```

```python
import functools

import jax
import jax.numpy as jnp
from jax import lax
from jax.experimental import pallas as pl
from jax.experimental.pallas import tpu as pltpu
from jax.sharding import PartitionSpec as P

MESH = pl.DeviceIdType.MESH
F32 = jnp.float32
BF16 = jnp.bfloat16
HEAD_DIM = 64
STATE_DIM = 128
NYC = 8
STATE_CHUNKS = 2
UNITS = 48
eps = 1e-06


def rms_scale(values, norm_gain):
    squares = jnp.mean(values * values, axis=-1, keepdims=True)
    return values * lax.rsqrt(squares + eps) * norm_gain


def dot(a, b):
    return jnp.dot(a, b, preferred_element_type=F32)


def two_terms(v):
    high = v.astype(BF16).astype(F32)
    return high, (v - high).astype(BF16).astype(F32)


def dot_rows(a, b):
    return lax.dot_general(a, b, (((1,), (1,)), ((), ())), preferred_element_type=F32)


def layer_kernel(
    n_ep,
    n_tp,
    tokens_hbm,
    mixer_gain_hbm,
    step_weight_hbm,
    step_bias_hbm,
    decay_log_hbm,
    skip_hbm,
    inner_kernel_hbm,
    state_kernel_hbm,
    inner_window_hbm,
    state_window_hbm,
    group_gain_hbm,
    gain_hbm,
    routes_hbm,
    route_weights_hbm,
    dense_gate_hbm,
    dense_up_hbm,
    dense_down_hbm,
    dense_scale_hbm,
    gate_weight_hbm,
    inner_weight_hbm,
    state_weight_hbm,
    output_weight_hbm,
    state_hbm,
    gate_hbm,
    up_hbm,
    down_hbm,
    out_ref,
    new_inner_ref,
    new_state_window_ref,
    new_state_ref,
    gate_w,
    inner_w,
    state_w,
    output_w,
    decay_rows,
    w_gate,
    w_up,
    w_down,
    parts,
    residual_ref,
    ffn_ref,
    dw,
    dx,
    combine_ref,
    tall,
    going,
    came,
    xs,
    act,
    dz_going,
    dz_came,
    hid,
    moe_going,
    moe_came,
    tall_back,
    back_going,
    back_came,
    od_going,
    od_came,
    tokens_ref,
    mixer_gain_ref,
    step_weight_ref,
    step_bias_ref,
    decay_log_ref,
    skip_ref,
    inner_kernel_ref,
    state_kernel_ref,
    inner_window_ref,
    state_window_ref,
    group_gain_ref,
    early_sems,
    gain_ref,
    routes_ref,
    route_weights_ref,
    dense_gate_ref,
    dense_up_ref,
    dense_down_ref,
    dense_scale_ref,
    late_sems,
    in_sems,
    state_sems,
    local_sems,
    send_sems,
    recv_sems,
    rounds,
):
    me = lax.axis_index("ep")
    t = lax.axis_index("tp")
    n_z = n_ep // NYC
    z = me // NYC
    yc = me % NYC
    seqs = tokens_ref.shape[0]
    heads = new_state_ref.shape[1]
    chunk = seqs // STATE_CHUNKS
    width = out_ref.shape[1]
    slots = 2 * n_ep

    def across_tp(k):
        return (me, lax.rem(t + k, n_tp))

    def along_z(k):
        return (lax.rem(z + k, n_z) * NYC + yc, t)

    def within_z(k):
        return (z * NYC + lax.rem(yc + k, NYC), t)

    def along_ep(kz, k):
        return (lax.rem(z + kz, n_z) * NYC + lax.rem(yc + k, NYC), t)

    steps = sorted(range(n_z), key=lambda kz: -min(kz, n_z - kz))

    def to_all(send, steps=steps):
        for kz in steps:
            for k in range(0 if kz else 1, NYC):
                send(kz, along_ep(kz, k))

    def remote(src, dst, which, peer):
        return pltpu.make_async_remote_copy(
            src_ref=src,
            dst_ref=dst,
            send_sem=send_sems.at[which],
            recv_sem=recv_sems.at[which],
            device_id=peer,
            device_id_type=MESH,
        )

    def wait_in(ref, which):
        remote(ref, ref, which, across_tp(1)).wait_recv()

    def wait_out(ref, which):
        remote(ref, ref, which, across_tp(1)).wait_send()

    PART, DW, DW2, DX, OUT, DZ, HID, MOE, MOE2, BACK, OD = range(11)

    early_loads = [
        pltpu.make_async_copy(src, dst, early_sems.at[i])
        for i, (src, dst) in enumerate(
            [
                (tokens_hbm, tokens_ref),
                (mixer_gain_hbm, mixer_gain_ref),
                (step_weight_hbm, step_weight_ref),
                (step_bias_hbm, step_bias_ref),
                (decay_log_hbm, decay_log_ref),
                (skip_hbm, skip_ref),
                (inner_kernel_hbm, inner_kernel_ref),
                (state_kernel_hbm, state_kernel_ref),
                (inner_window_hbm, inner_window_ref),
                (state_window_hbm, state_window_ref),
                (group_gain_hbm, group_gain_ref),
            ]
        )
    ]
    for load in early_loads:
        load.start()
    mixer_loads = [
        pltpu.make_async_copy(src, dst, in_sems.at[i])
        for i, (src, dst) in enumerate(
            [
                (inner_weight_hbm, inner_w),
                (state_weight_hbm, state_w),
                (gate_weight_hbm, gate_w),
                (output_weight_hbm, output_w),
            ]
        )
    ]
    for load in mixer_loads[:3]:
        load.start()

    barrier = pltpu.get_barrier_semaphore()
    for k in range(1, n_tp):
        pl.semaphore_signal(barrier, inc=1, device_id=across_tp(k), device_id_type=MESH)

    for k in range(1, NYC):
        pl.semaphore_signal(barrier, inc=1, device_id=within_z(k), device_id_type=MESH)
    for k in (1, n_z - 1):
        pl.semaphore_signal(barrier, inc=1, device_id=along_z(k), device_id_type=MESH)

    state_loads = [
        pltpu.make_async_copy(
            state_hbm.at[pl.ds(c * chunk, chunk)], new_state_ref.at[pl.ds(c * chunk, chunk)], state_sems.at[c]
        )
        for c in range(STATE_CHUNKS)
    ]
    for load in state_loads:
        load.start()
    mixer_loads[3].start()
    late_loads = [
        pltpu.make_async_copy(src, dst, late_sems.at[i])
        for i, (src, dst) in enumerate(
            [
                (gain_hbm, gain_ref),
                (routes_hbm, routes_ref),
                (route_weights_hbm, route_weights_ref),
                (dense_gate_hbm, dense_gate_ref),
                (dense_up_hbm, dense_up_ref),
                (dense_down_hbm, dense_down_ref),
                (dense_scale_hbm, dense_scale_ref),
            ]
        )
    ]
    for load in late_loads:
        load.start()
    for load in early_loads[:2]:
        load.wait()

    normed = rms_scale(tokens_ref[...].astype(F32), mixer_gain_ref[...]).astype(BF16)
    for load in early_loads[2:]:
        load.wait()
    step_raw = dot_rows(normed, step_weight_ref[...])
    step_in = step_raw + step_bias_ref[...]
    step = jnp.maximum(step_in, 0.0) + jnp.log1p(jnp.exp(-jnp.abs(step_in)))
    decay = jnp.exp(-step * jnp.exp(decay_log_ref[...]))

    for load in mixer_loads[:3]:
        load.wait()
    inner_pre = dot(normed, inner_w[...]).astype(BF16).astype(F32)
    kern = inner_kernel_ref[...]
    conv = inner_pre * kern[3:4]
    for j in range(3):
        conv = conv + inner_window_ref[j].astype(F32) * kern[j : j + 1]
    inner = jax.nn.silu(conv)
    new_inner_ref[0:2] = inner_window_ref[1:3]
    new_inner_ref[2] = inner_pre.astype(BF16)

    vectors = []
    pres = []
    for r in range(2):
        pre = dot(normed, state_w[r]).astype(BF16).astype(F32)
        conv = pre * state_kernel_ref[3, r : r + 1, :]
        for j in range(3):
            conv = conv + state_window_ref[:, j, r, :].astype(F32) * state_kernel_ref[j, r : r + 1, :]
        vectors.append(jax.nn.silu(conv))
        pres.append(pre)
    new_state_window_ref[:, 0:2] = state_window_ref[:, 1:3]
    new_state_window_ref[:, 2] = jnp.concatenate(
        [pres[0][:, None, :], pres[1][:, None, :]], axis=1
    ).astype(BF16)
    in_vector, out_vector = vectors

    gate_pre = dot(normed, gate_w[...])

    lane = lax.broadcasted_iota(jnp.int32, inner.shape, 1) // HEAD_DIM

    def widen(v):
        wide = jnp.broadcast_to(v[:, 0:1], inner.shape)
        for h in range(1, heads):
            wide = jnp.where(lane == h, v[:, h : h + 1], wide)
        return wide

    spare = jnp.zeros((32 - seqs, STATE_DIM), F32)
    high, low = two_terms(jnp.concatenate([out_vector, spare], axis=0))
    reader = jnp.transpose(
        jnp.concatenate([high, low, jnp.zeros((64, STATE_DIM), F32)], axis=0)
    ).astype(BF16)
    read = jnp.zeros((width, STATE_DIM), F32)
    column = lax.broadcasted_iota(jnp.int32, (width, STATE_DIM), 1) % 32
    written_rows = widen(step) * inner
    fresh = written_rows * jnp.sum(in_vector * out_vector, axis=1, keepdims=True)
    fresh = fresh + widen(skip_ref[...]) * inner
    decay_wide = widen(decay)
    opened = jax.nn.silu(gate_pre)

    pl.semaphore_wait(barrier, n_tp - 1 + NYC - 1 + 2)
    for k in (1, n_z - 1):
        pl.semaphore_signal(rounds.at[0], inc=1, device_id=along_z(k), device_id_type=MESH)

    for k in range(STATE_CHUNKS):
        state_loads[k].wait()
        olds = new_state_ref[k * chunk : (k + 1) * chunk].reshape(chunk * width, STATE_DIM)
        found = dot(olds.astype(BF16), reader)
        for i in range(chunk):
            read = jnp.where(column == k * chunk + i, found[i * width : (i + 1) * width], read)
    pl.semaphore_wait(rounds.at[0], 2)
    for k in (2, n_z - 2):
        pl.semaphore_signal(rounds.at[1], inc=1, device_id=along_z(k), device_id_type=MESH)

    mixed = jnp.transpose(read)
    gated = (decay_wide * (mixed[:seqs] + mixed[32 : 32 + seqs]) + fresh) * opened
    mixer_rows = (rms_scale(gated, 1.0) * group_gain_ref[...]).astype(BF16)
    mixer_loads[3].wait()
    parts[t] = dot(mixer_rows, output_w[...]).astype(BF16)

    for k in range(1, n_tp):
        remote(parts.at[t], parts.at[t], PART, across_tp(k)).start()

    for load in late_loads:
        load.wait()
    units = dense_gate_ref.shape[0]
    gap = jnp.zeros((UNITS - units, width), F32)
    for i, ref in enumerate((dense_gate_ref, dense_up_ref, dense_down_ref)):
        dw[yc, i * UNITS : (i + 1) * UNITS] = jnp.concatenate(
            [ref[...].astype(F32), gap], axis=0
        ).astype(BF16)

    for k in range(2, NYC, 2):
        remote(dw.at[yc], dw.at[yc], DW, within_z(k)).start()

    expert = lax.broadcasted_iota(jnp.int32, (n_ep, seqs), 0)
    named = [(routes_ref[k : k + 1, :] == expert).astype(F32) for k in range(2)]
    earlier = (
        lax.broadcasted_iota(jnp.int32, (seqs, seqs), 0)
        < lax.broadcasted_iota(jnp.int32, (seqs, seqs), 1)
    ).astype(F32)
    before = dot(named[0] + named[1], earlier)
    place = lax.broadcasted_iota(jnp.int32, (slots, seqs), 0)
    chosen = []
    for k in range(2):
        slot = jnp.sum(before * named[k], axis=0, keepdims=True).astype(jnp.int32)
        chosen.append((place == routes_ref[k : k + 1, :] * 2 + slot).astype(F32))
    selection = (chosen[0] + chosen[1]).astype(BF16)
    combine_ref[...] = jnp.transpose(
        chosen[0] * route_weights_ref[0:1, :] + chosen[1] * route_weights_ref[1:2, :]
    )

    loads = [
        pltpu.make_async_copy(src.at[0], dst, local_sems.at[i])
        for i, (src, dst) in enumerate([(gate_hbm, w_gate), (up_hbm, w_up), (down_hbm, w_down)])
    ]
    for load in loads:
        load.start()

    pl.semaphore_wait(rounds.at[1], 2)
    for k in range(1, NYC):
        pl.semaphore_signal(rounds.at[2], inc=1, device_id=within_z(k), device_id_type=MESH)

    for h in range(heads):
        decay_rows[:, h * STATE_DIM : (h + 1) * STATE_DIM] = jnp.broadcast_to(
            decay[:, h : h + 1], (seqs, STATE_DIM)
        )
    high, low = two_terms(
        jnp.concatenate([written_rows, jnp.zeros((32 - seqs, width), F32)], axis=0)
    )
    written = jnp.transpose(
        jnp.concatenate([high, high, low, jnp.zeros_like(low)], axis=0)
    ).astype(BF16)
    high, low = two_terms(jnp.concatenate([in_vector, spare], axis=0))
    inputs = jnp.concatenate([high, low, high, jnp.zeros_like(low)], axis=0)
    owner = lax.broadcasted_iota(jnp.int32, inputs.shape, 0) % 32
    for first in range(0, seqs, 2):
        pair = (first, first + 1)
        added = dot(
            written,
            jnp.concatenate([jnp.where(owner == b, inputs, 0.0) for b in pair], axis=1).astype(BF16),
        )
        for n, b in enumerate(pair):
            rates = decay_rows[b : b + 1, :]
            for h in range(heads):
                new_state_ref[b, h] = new_state_ref[b, h] * rates[:, h * STATE_DIM : (h + 1) * STATE_DIM] + (
                    added[h * HEAD_DIM : (h + 1) * HEAD_DIM, n * STATE_DIM : (n + 1) * STATE_DIM]
                )

    wait_in(parts.at[pl.ds(0, n_tp - 1)], PART)
    total = parts[0].astype(F32)
    for k in range(1, n_tp):
        total = total + parts[k].astype(F32)
    residual = tokens_ref[...].astype(F32) + total
    residual_ref[...] = residual
    ffn = rms_scale(residual, gain_ref[...]).astype(BF16)
    ffn_ref[...] = ffn

    own = pl.ds(pl.multiple_of(t * width, width), width)
    dx[z] = ffn_ref[:, own]

    for k in steps[:-1]:
        remote(dx.at[z], dx.at[z], DX, along_z(k)).start()

    outgoing = dot(selection, ffn)
    lines = outgoing.shape[1] // 128
    for j in range(lines):
        tall[pl.ds(j, slots, stride=lines), :] = outgoing[:, j * 128 : (j + 1) * 128]
    going[...] = tall[...].reshape(going.shape).astype(BF16)

    pl.semaphore_wait(rounds.at[2], NYC - 1)
    def dispatch(kz, peer):
        place = steps.index((n_z - kz) % n_z) * NYC + yc
        remote(going.at[peer[0]], came.at[place], OUT, peer).start()

    to_all(dispatch)
    came[(n_z - 1) * NYC + yc] = going[me]

    wait_in(dw.at[pl.ds(0, NYC // 2 - 1)], DW)
    sibling = (z * NYC + yc + 1 - 2 * lax.rem(yc, 2), t)
    for k in range(0, NYC, 2):
        held = lax.rem(yc + k, NYC)
        remote(dw.at[held], dw.at[held], DW2, sibling).start()
    wait_in(dw.at[pl.ds(0, NYC // 2)], DW2)
    wait_in(dx.at[pl.ds(0, n_z - 1)], DX)
    dense_rows = dx[...].reshape(n_z * seqs, width)
    for i in range(2):
        weights = dw[:, i * UNITS : (i + 1) * UNITS].reshape(NYC * UNITS, width)
        dz_going[:, :, i * NYC * UNITS : (i + 1) * NYC * UNITS] = (
            dot_rows(dense_rows, weights).astype(BF16).reshape(n_tp, -1, NYC * UNITS)
        )
    for k in range(1, n_tp):
        peer = across_tp(k)
        remote(dz_going.at[peer[1]], dz_came.at[t], DZ, peer).start()
    dz_came[t] = dz_going[t]

    wait_in(came.at[pl.ds(0, n_ep - 1)], OUT)
    tall[...] = came[...].astype(F32).reshape(tall.shape)
    for j in range(lines):
        xs[:, j * 128 : (j + 1) * 128] = tall[pl.ds(j, slots, stride=lines), :].astype(BF16)
    loads[0].wait()
    loads[1].wait()
    rows = xs[...]
    act[...] = (jax.nn.silu(dot_rows(rows, w_gate[...])) * dot_rows(rows, w_up[...])).astype(BF16)
    loads[2].wait()
    halves = [pl.ds(0, n_ep), pl.ds(n_ep, n_ep)]
    for k in range(1, n_tp):
        peer = across_tp(k)
        columns = pl.ds(pl.multiple_of(peer[1] * width, width), width)
        moe_going[peer[1]] = dot(act[...], w_down[:, columns]).astype(BF16)
        half = (peer[1], halves[0])
        remote(moe_going.at[half], moe_came.at[t, halves[0]], MOE, peer).start()
    for k in range(1, n_tp):
        peer = across_tp(k)
        half = (peer[1], halves[1])
        remote(moe_going.at[half], moe_came.at[t, halves[1]], MOE2, peer).start()
    moe_came[t] = dot(act[...], w_down[:, own]).astype(BF16)

    wait_in(dz_came.at[pl.ds(0, n_tp - 1)], DZ)
    gate_up = dz_came[0].astype(F32)
    for k in range(1, n_tp):
        gate_up = gate_up + dz_came[k].astype(F32)
    hid[t] = (
        jax.nn.silu(gate_up[:, : NYC * UNITS]) * gate_up[:, NYC * UNITS :]
    ).astype(BF16)
    for k in range(1, n_tp):
        remote(hid.at[t], hid.at[t], HID, across_tp(k)).start()

    for n, which in enumerate((MOE, MOE2)):
        wait_in(moe_came.at[pl.ds(0, n_tp - 1), halves[n]], which)
        rows_out = moe_came[0, halves[n]].astype(F32)
        for k in range(1, n_tp):
            rows_out = rows_out + moe_came[k, halves[n]].astype(F32)
        lines = pl.ds(n * slots, slots)
        for j in range(width // 128):
            tall_back[pl.ds(n * slots + j, n_ep, stride=2), :] = rows_out[:, j * 128 : (j + 1) * 128]
        back_going[pl.ds(n * n_ep // 2, n_ep // 2)] = (
            tall_back[lines].reshape(n_ep // 2, 4, 128).astype(BF16)
        )

        def give_back(kz, peer):
            place = steps.index(kz) * NYC + peer[0] % NYC
            remote(back_going.at[place], back_came.at[me], BACK, peer).start()

        to_all(give_back, steps[n * n_z // 2 : (n + 1) * n_z // 2])
    back_came[me] = back_going[(n_z - 1) * NYC + yc]

    wait_in(hid.at[pl.ds(0, n_tp - 1)], HID)
    dense_part = dot(
        hid[...].reshape(n_z * seqs, NYC * UNITS),
        dw[:, 2 * UNITS : 3 * UNITS].reshape(NYC * UNITS, width),
    )
    od_going[...] = dense_part.astype(BF16).reshape(od_going.shape)

    for k in steps[:-1]:
        there = lax.rem(z + k, n_z)
        remote(od_going.at[there], od_came.at[z], OD, along_z(k)).start()
    od_came[z] = od_going[z]

    wait_in(od_came.at[pl.ds(0, n_z - 1)], OD)
    dense_out = od_came[0].astype(F32)
    for k in range(1, n_z):
        dense_out = dense_out + od_came[k].astype(F32)

    wait_in(back_came.at[pl.ds(0, n_ep - 1)], BACK)
    tall_back[...] = back_came[...].astype(F32).reshape(tall_back.shape)
    returned = [
        tall_back[pl.ds(j, slots, stride=2), :].astype(BF16) for j in range(width // 128)
    ]
    returned = jnp.concatenate(returned, axis=1).astype(F32)
    expert_out = jnp.dot(combine_ref[...], returned, precision=lax.Precision.HIGHEST)
    out_ref[...] = (
        residual_ref[:, own] + expert_out + dense_scale_ref[...] * dense_out
    ).astype(BF16)

    wait_out(parts.at[pl.ds(0, n_tp - 1)], PART)
    wait_out(dw.at[pl.ds(0, NYC // 2 - 1)], DW)
    wait_out(dw.at[pl.ds(0, NYC // 2)], DW2)
    wait_out(dx.at[pl.ds(0, n_z - 1)], DX)
    wait_out(going.at[pl.ds(0, n_ep - 1)], OUT)
    wait_out(dz_going.at[pl.ds(0, n_tp - 1)], DZ)
    wait_out(hid.at[pl.ds(0, n_tp - 1)], HID)
    wait_out(moe_going.at[pl.ds(0, n_tp - 1), halves[0]], MOE)
    wait_out(moe_going.at[pl.ds(0, n_tp - 1), halves[1]], MOE2)
    wait_out(back_going.at[pl.ds(0, n_ep - 1)], BACK)
    wait_out(od_going.at[pl.ds(0, n_z - 1)], OD)


def write_kernel(*refs):
    sems = refs[-1]
    copies = [pltpu.make_async_copy(refs[i], refs[4 + i], sems.at[i]) for i in (3, 0, 1, 2)]
    for copy in copies:
        copy.start()
    for copy in copies:
        copy.wait()


VMEM = pl.BlockSpec(memory_space=pltpu.VMEM)
ANY = pl.BlockSpec(memory_space=pl.ANY)


def local(
    n_ep,
    n_tp,
    tokens,
    mixer_gain,
    gate_weight,
    inner_weight,
    state_weight,
    step_weight,
    step_bias,
    decay_log,
    skip_scale,
    inner_kernel,
    state_kernel,
    inner_window,
    state_window,
    recurrent_state,
    group_gain,
    output_weight,
    channel_gain,
    routes,
    route_weights,
    expert_gate,
    expert_up,
    expert_down,
    dense_gate,
    dense_up,
    dense_down,
    dense_scale,
):
    seqs, model = tokens.shape
    width = dense_scale.shape[0]
    hidden = expert_gate.shape[2]
    n_z = n_ep // NYC
    slots = 2 * n_ep
    early = (
        tokens,
        mixer_gain[None],
        step_weight.T,
        step_bias[None],
        decay_log[None],
        skip_scale[None],
        inner_kernel,
        state_kernel,
        jnp.swapaxes(inner_window, 0, 1),
        state_window,
        group_gain[None],
    )
    late = (
        channel_gain[None],
        routes.T,
        route_weights.T,
        dense_gate.T,
        dense_up.T,
        dense_down,
        dense_scale[None],
    )
    scratch = [
        pltpu.VMEM(gate_weight.shape, BF16),
        pltpu.VMEM(inner_weight.shape, BF16),
        pltpu.VMEM(state_weight.shape, BF16),
        pltpu.VMEM(output_weight.shape, BF16),
        pltpu.VMEM((seqs, step_bias.shape[0] * STATE_DIM), F32),
        pltpu.VMEM((hidden, model), BF16),
        pltpu.VMEM((hidden, model), BF16),
        pltpu.VMEM((hidden, model), BF16),
        pltpu.VMEM((n_tp, seqs, model), BF16),
        pltpu.VMEM((seqs, model), F32),
        pltpu.VMEM((seqs, model), BF16),
        pltpu.VMEM((NYC, 3 * UNITS, width), BF16),
        pltpu.VMEM((n_z, seqs, width), BF16),
        pltpu.VMEM((seqs, slots), F32),
        pltpu.VMEM((slots * model // 128, 128), F32),
        pltpu.VMEM((n_ep, 2 * model // 128, 128), BF16),
        pltpu.VMEM((n_ep, 2 * model // 128, 128), BF16),
        pltpu.VMEM((slots, model), BF16),
        pltpu.VMEM((slots, hidden), BF16),
        pltpu.VMEM((n_tp, n_z * seqs // n_tp, 2 * NYC * UNITS), BF16),
        pltpu.VMEM((n_tp, n_z * seqs // n_tp, 2 * NYC * UNITS), BF16),
        pltpu.VMEM((n_tp, n_z * seqs // n_tp, NYC * UNITS), BF16),
        pltpu.VMEM((n_tp, slots, width), BF16),
        pltpu.VMEM((n_tp, slots, width), BF16),
        pltpu.VMEM((slots * 2, 128), F32),
        pltpu.VMEM((n_ep, 4, 128), BF16),
        pltpu.VMEM((n_ep, 4, 128), BF16),
        pltpu.VMEM((n_z, seqs, width), BF16),
        pltpu.VMEM((n_z, seqs, width), BF16),
        *[pltpu.VMEM(x.shape, x.dtype) for x in early],
        pltpu.SemaphoreType.DMA((len(early),)),
        *[pltpu.VMEM(x.shape, x.dtype) for x in late],
        pltpu.SemaphoreType.DMA((len(late),)),
        pltpu.SemaphoreType.DMA((4,)),
        pltpu.SemaphoreType.DMA((4,)),
        pltpu.SemaphoreType.DMA((3,)),
        pltpu.SemaphoreType.DMA((11,)),
        pltpu.SemaphoreType.DMA((11,)),
        pltpu.SemaphoreType.REGULAR((3,)),
    ]
    results = [
        ((seqs, width), BF16),
        ((3, seqs, width), BF16),
        (state_window.shape, BF16),
        (recurrent_state.shape, F32),
    ]
    held = pl.pallas_call(
        functools.partial(layer_kernel, n_ep, n_tp),
        out_shape=tuple(pltpu.VMEM(*r) for r in results),
        in_specs=[ANY] * 26,
        out_specs=(VMEM,) * 4,
        scratch_shapes=scratch,
        compiler_params=pltpu.CompilerParams(collective_id=0, has_side_effects=True),
        name="layer",
    )(
        *early,
        *late,
        gate_weight,
        inner_weight,
        state_weight,
        output_weight,
        recurrent_state,
        jnp.swapaxes(expert_gate, 1, 2),
        jnp.swapaxes(expert_up, 1, 2),
        expert_down,
    )
    new_tokens, new_inner, new_window, new_state = pl.pallas_call(
        write_kernel,
        out_shape=tuple(jax.ShapeDtypeStruct(*r) for r in results),
        in_specs=[VMEM] * 4,
        out_specs=(ANY,) * 4,
        scratch_shapes=[pltpu.SemaphoreType.DMA((4,))],
        name="write",
    )(*(pltpu.with_memory_space_constraint(h, pltpu.VMEM) for h in held))
    return new_tokens, new_state, jnp.swapaxes(new_inner, 0, 1), new_window


def solution(mesh):
    placed = (
        P("ep", None),
        P(),
        P(None, "tp"),
        P(None, "tp"),
        P(None, None, "tp"),
        P(None, "tp"),
        P("tp"),
        P("tp"),
        P("tp"),
        P(None, "tp"),
        P(None, None, "tp"),
        P("ep", None, "tp"),
        P("ep", None, None, "tp"),
        P("ep", "tp", None, None),
        P("tp"),
        P("tp", None),
        P(),
        P("ep", None),
        P("ep", None),
        P("ep", None, "tp"),
        P("ep", None, "tp"),
        P("ep", "tp", None),
        P("tp", "ep"),
        P("tp", "ep"),
        P("ep", "tp"),
        P("tp"),
    )
    return jax.shard_map(
        functools.partial(local, mesh.shape["ep"], mesh.shape["tp"]),
        mesh=mesh,
        in_specs=placed,
        out_specs=(
            P("ep", "tp"),
            P("ep", "tp", None, None),
            P("ep", None, "tp"),
            P("ep", None, None, "tp"),
        ),
        check_vma=False,
    )
```

```python
import functools

import jax
import jax.numpy as jnp
from jax import lax
from jax.experimental import pallas as pl
from jax.experimental.pallas import tpu as pltpu
from jax.sharding import PartitionSpec as P

MESH = pl.DeviceIdType.MESH
F32 = jnp.float32
BF16 = jnp.bfloat16
HEAD_DIM = 64
STATE_DIM = 128
NYC = 8
STATE_CHUNKS = 2
UNITS = 48
eps = 1e-06


def rms_scale(values, norm_gain):
    squares = jnp.mean(values * values, axis=-1, keepdims=True)
    return values * lax.rsqrt(squares + eps) * norm_gain


def dot(a, b):
    return jnp.dot(a, b, preferred_element_type=F32)


def two_terms(v):
    high = v.astype(BF16).astype(F32)
    return high, (v - high).astype(BF16).astype(F32)


def dot_rows(a, b):
    return lax.dot_general(a, b, (((1,), (1,)), ((), ())), preferred_element_type=F32)


def layer_kernel(
    n_ep,
    n_tp,
    tokens_hbm,
    mixer_gain_hbm,
    step_weight_hbm,
    step_bias_hbm,
    decay_log_hbm,
    skip_hbm,
    inner_kernel_hbm,
    state_kernel_hbm,
    inner_window_hbm,
    state_window_hbm,
    group_gain_hbm,
    gain_hbm,
    routes_hbm,
    route_weights_hbm,
    dense_gate_hbm,
    dense_up_hbm,
    dense_down_hbm,
    dense_scale_hbm,
    gate_weight_hbm,
    inner_weight_hbm,
    state_weight_hbm,
    output_weight_hbm,
    state_hbm,
    gate_hbm,
    up_hbm,
    down_hbm,
    out_ref,
    new_inner_ref,
    new_state_window_ref,
    new_state_ref,
    gate_w,
    inner_w,
    state_w,
    output_w,
    decay_rows,
    w_gate,
    w_up,
    w_down,
    parts,
    residual_ref,
    ffn_ref,
    dw,
    dx,
    combine_ref,
    tall,
    going,
    came,
    xs,
    act,
    dz_going,
    dz_came,
    hid,
    moe_going,
    moe_came,
    tall_back,
    back_going,
    back_came,
    od_going,
    od_came,
    tokens_ref,
    mixer_gain_ref,
    step_weight_ref,
    step_bias_ref,
    decay_log_ref,
    skip_ref,
    inner_kernel_ref,
    state_kernel_ref,
    inner_window_ref,
    state_window_ref,
    group_gain_ref,
    early_sems,
    gain_ref,
    routes_ref,
    route_weights_ref,
    dense_gate_ref,
    dense_up_ref,
    dense_down_ref,
    dense_scale_ref,
    late_sems,
    in_sems,
    state_sems,
    local_sems,
    send_sems,
    recv_sems,
    rounds,
):
    me = lax.axis_index("ep")
    t = lax.axis_index("tp")
    n_z = n_ep // NYC
    z = me // NYC
    yc = me % NYC
    seqs = tokens_ref.shape[0]
    heads = new_state_ref.shape[1]
    chunk = seqs // STATE_CHUNKS
    width = out_ref.shape[1]
    slots = 2 * n_ep

    def across_tp(k):
        return (me, lax.rem(t + k, n_tp))

    def along_z(k):
        return (lax.rem(z + k, n_z) * NYC + yc, t)

    def within_z(k):
        return (z * NYC + lax.rem(yc + k, NYC), t)

    def along_ep(kz, k):
        return (lax.rem(z + kz, n_z) * NYC + lax.rem(yc + k, NYC), t)

    steps = sorted(range(n_z), key=lambda kz: -min(kz, n_z - kz))

    def to_all(send, steps=steps):
        for kz in steps:
            for k in range(0 if kz else 1, NYC):
                send(kz, along_ep(kz, k))

    def remote(src, dst, which, peer):
        return pltpu.make_async_remote_copy(
            src_ref=src,
            dst_ref=dst,
            send_sem=send_sems.at[which],
            recv_sem=recv_sems.at[which],
            device_id=peer,
            device_id_type=MESH,
        )

    def wait_in(ref, which):
        remote(ref, ref, which, across_tp(1)).wait_recv()

    def wait_out(ref, which):
        remote(ref, ref, which, across_tp(1)).wait_send()

    PART, DW, DW2, DX, OUT, DZ, HID, MOE, MOE2, BACK, OD = range(11)

    early_loads = [
        pltpu.make_async_copy(src, dst, early_sems.at[i])
        for i, (src, dst) in enumerate(
            [
                (tokens_hbm, tokens_ref),
                (mixer_gain_hbm, mixer_gain_ref),
                (step_weight_hbm, step_weight_ref),
                (step_bias_hbm, step_bias_ref),
                (decay_log_hbm, decay_log_ref),
                (skip_hbm, skip_ref),
                (inner_kernel_hbm, inner_kernel_ref),
                (state_kernel_hbm, state_kernel_ref),
                (inner_window_hbm, inner_window_ref),
                (state_window_hbm, state_window_ref),
                (group_gain_hbm, group_gain_ref),
            ]
        )
    ]
    for load in early_loads:
        load.start()
    mixer_loads = [
        pltpu.make_async_copy(src, dst, in_sems.at[i])
        for i, (src, dst) in enumerate(
            [
                (inner_weight_hbm, inner_w),
                (state_weight_hbm, state_w),
                (gate_weight_hbm, gate_w),
                (output_weight_hbm, output_w),
            ]
        )
    ]
    for load in mixer_loads[:3]:
        load.start()

    barrier = pltpu.get_barrier_semaphore()
    for k in range(1, n_tp):
        pl.semaphore_signal(barrier, inc=1, device_id=across_tp(k), device_id_type=MESH)

    for k in range(1, NYC):
        pl.semaphore_signal(barrier, inc=1, device_id=within_z(k), device_id_type=MESH)
    for k in (1, n_z - 1):
        pl.semaphore_signal(barrier, inc=1, device_id=along_z(k), device_id_type=MESH)

    state_loads = [
        pltpu.make_async_copy(
            state_hbm.at[pl.ds(c * chunk, chunk)], new_state_ref.at[pl.ds(c * chunk, chunk)], state_sems.at[c]
        )
        for c in range(STATE_CHUNKS)
    ]
    for load in state_loads:
        load.start()
    mixer_loads[3].start()
    late_loads = [
        pltpu.make_async_copy(src, dst, late_sems.at[i])
        for i, (src, dst) in enumerate(
            [
                (gain_hbm, gain_ref),
                (routes_hbm, routes_ref),
                (route_weights_hbm, route_weights_ref),
                (dense_gate_hbm, dense_gate_ref),
                (dense_up_hbm, dense_up_ref),
                (dense_down_hbm, dense_down_ref),
                (dense_scale_hbm, dense_scale_ref),
            ]
        )
    ]
    for load in late_loads:
        load.start()
    for load in early_loads[:2]:
        load.wait()

    normed = rms_scale(tokens_ref[...].astype(F32), mixer_gain_ref[...]).astype(BF16)
    for load in early_loads[2:]:
        load.wait()
    step_raw = dot_rows(normed, step_weight_ref[...])
    step_in = step_raw + step_bias_ref[...]
    step = jnp.maximum(step_in, 0.0) + jnp.log1p(jnp.exp(-jnp.abs(step_in)))
    decay = jnp.exp(-step * jnp.exp(decay_log_ref[...]))

    for load in mixer_loads[:2]:
        load.wait()
    inner_pre = dot(normed, inner_w[...]).astype(BF16).astype(F32)
    kern = inner_kernel_ref[...]
    conv = inner_pre * kern[3:4]
    for j in range(3):
        conv = conv + inner_window_ref[j].astype(F32) * kern[j : j + 1]
    inner = jax.nn.silu(conv)
    new_inner_ref[0:2] = inner_window_ref[1:3]
    new_inner_ref[2] = inner_pre.astype(BF16)

    vectors = []
    pres = []
    for r in range(2):
        pre = dot(normed, state_w[r]).astype(BF16).astype(F32)
        conv = pre * state_kernel_ref[3, r : r + 1, :]
        for j in range(3):
            conv = conv + state_window_ref[:, j, r, :].astype(F32) * state_kernel_ref[j, r : r + 1, :]
        vectors.append(jax.nn.silu(conv))
        pres.append(pre)
    new_state_window_ref[:, 0:2] = state_window_ref[:, 1:3]
    new_state_window_ref[:, 2] = jnp.concatenate(
        [pres[0][:, None, :], pres[1][:, None, :]], axis=1
    ).astype(BF16)
    in_vector, out_vector = vectors

    mixer_loads[2].wait()
    gate_pre = dot(normed, gate_w[...])

    lane = lax.broadcasted_iota(jnp.int32, inner.shape, 1) // HEAD_DIM

    def widen(v):
        wide = jnp.broadcast_to(v[:, 0:1], inner.shape)
        for h in range(1, heads):
            wide = jnp.where(lane == h, v[:, h : h + 1], wide)
        return wide

    spare = jnp.zeros((32 - seqs, STATE_DIM), F32)
    high, low = two_terms(jnp.concatenate([out_vector, spare], axis=0))
    reader = jnp.transpose(
        jnp.concatenate([high, low, jnp.zeros((64, STATE_DIM), F32)], axis=0)
    ).astype(BF16)
    read = jnp.zeros((width, STATE_DIM), F32)
    column = lax.broadcasted_iota(jnp.int32, (width, STATE_DIM), 1) % 32
    written_rows = widen(step) * inner
    fresh = written_rows * jnp.sum(in_vector * out_vector, axis=1, keepdims=True)
    fresh = fresh + widen(skip_ref[...]) * inner
    decay_wide = widen(decay)
    opened = jax.nn.silu(gate_pre)

    pl.semaphore_wait(barrier, n_tp - 1 + NYC - 1 + 2)
    for k in (1, n_z - 1):
        pl.semaphore_signal(rounds.at[0], inc=1, device_id=along_z(k), device_id_type=MESH)

    for k in range(STATE_CHUNKS):
        state_loads[k].wait()
        olds = new_state_ref[k * chunk : (k + 1) * chunk].reshape(chunk * width, STATE_DIM)
        found = dot(olds.astype(BF16), reader)
        for i in range(chunk):
            read = jnp.where(column == k * chunk + i, found[i * width : (i + 1) * width], read)
    pl.semaphore_wait(rounds.at[0], 2)
    for k in (2, n_z - 2):
        pl.semaphore_signal(rounds.at[1], inc=1, device_id=along_z(k), device_id_type=MESH)

    mixed = jnp.transpose(read)
    gated = (decay_wide * (mixed[:seqs] + mixed[32 : 32 + seqs]) + fresh) * opened
    mixer_rows = (rms_scale(gated, 1.0) * group_gain_ref[...]).astype(BF16)
    mixer_loads[3].wait()
    parts[t] = dot(mixer_rows, output_w[...]).astype(BF16)

    for k in range(1, n_tp):
        remote(parts.at[t], parts.at[t], PART, across_tp(k)).start()

    for load in late_loads:
        load.wait()
    units = dense_gate_ref.shape[0]
    gap = jnp.zeros((UNITS - units, width), F32)
    for i, ref in enumerate((dense_gate_ref, dense_up_ref, dense_down_ref)):
        dw[yc, i * UNITS : (i + 1) * UNITS] = jnp.concatenate(
            [ref[...].astype(F32), gap], axis=0
        ).astype(BF16)

    for k in range(2, NYC, 2):
        remote(dw.at[yc], dw.at[yc], DW, within_z(k)).start()

    expert = lax.broadcasted_iota(jnp.int32, (n_ep, seqs), 0)
    named = [(routes_ref[k : k + 1, :] == expert).astype(F32) for k in range(2)]
    earlier = (
        lax.broadcasted_iota(jnp.int32, (seqs, seqs), 0)
        < lax.broadcasted_iota(jnp.int32, (seqs, seqs), 1)
    ).astype(F32)
    before = dot(named[0] + named[1], earlier)
    place = lax.broadcasted_iota(jnp.int32, (slots, seqs), 0)
    chosen = []
    for k in range(2):
        slot = jnp.sum(before * named[k], axis=0, keepdims=True).astype(jnp.int32)
        chosen.append((place == routes_ref[k : k + 1, :] * 2 + slot).astype(F32))
    selection = (chosen[0] + chosen[1]).astype(BF16)
    combine_ref[...] = jnp.transpose(
        chosen[0] * route_weights_ref[0:1, :] + chosen[1] * route_weights_ref[1:2, :]
    )

    loads = [
        pltpu.make_async_copy(src.at[0], dst, local_sems.at[i])
        for i, (src, dst) in enumerate([(gate_hbm, w_gate), (up_hbm, w_up), (down_hbm, w_down)])
    ]
    for load in loads:
        load.start()

    pl.semaphore_wait(rounds.at[1], 2)
    for k in range(1, NYC):
        pl.semaphore_signal(rounds.at[2], inc=1, device_id=within_z(k), device_id_type=MESH)

    for h in range(heads):
        decay_rows[:, h * STATE_DIM : (h + 1) * STATE_DIM] = jnp.broadcast_to(
            decay[:, h : h + 1], (seqs, STATE_DIM)
        )
    high, low = two_terms(
        jnp.concatenate([written_rows, jnp.zeros((32 - seqs, width), F32)], axis=0)
    )
    written = jnp.transpose(
        jnp.concatenate([high, high, low, jnp.zeros_like(low)], axis=0)
    ).astype(BF16)
    high, low = two_terms(jnp.concatenate([in_vector, spare], axis=0))
    inputs = jnp.concatenate([high, low, high, jnp.zeros_like(low)], axis=0)
    owner = lax.broadcasted_iota(jnp.int32, inputs.shape, 0) % 32
    for first in range(0, seqs, 2):
        pair = (first, first + 1)
        added = dot(
            written,
            jnp.concatenate([jnp.where(owner == b, inputs, 0.0) for b in pair], axis=1).astype(BF16),
        )
        for n, b in enumerate(pair):
            rates = decay_rows[b : b + 1, :]
            for h in range(heads):
                new_state_ref[b, h] = new_state_ref[b, h] * rates[:, h * STATE_DIM : (h + 1) * STATE_DIM] + (
                    added[h * HEAD_DIM : (h + 1) * HEAD_DIM, n * STATE_DIM : (n + 1) * STATE_DIM]
                )

    wait_in(parts.at[pl.ds(0, n_tp - 1)], PART)
    total = parts[0].astype(F32)
    for k in range(1, n_tp):
        total = total + parts[k].astype(F32)
    residual = tokens_ref[...].astype(F32) + total
    residual_ref[...] = residual
    ffn = rms_scale(residual, gain_ref[...]).astype(BF16)
    ffn_ref[...] = ffn

    own = pl.ds(pl.multiple_of(t * width, width), width)
    dx[z] = ffn_ref[:, own]

    for k in steps[:-1]:
        remote(dx.at[z], dx.at[z], DX, along_z(k)).start()

    outgoing = dot(selection, ffn)
    lines = outgoing.shape[1] // 128
    for j in range(lines):
        tall[pl.ds(j, slots, stride=lines), :] = outgoing[:, j * 128 : (j + 1) * 128]
    going[...] = tall[...].reshape(going.shape).astype(BF16)

    pl.semaphore_wait(rounds.at[2], NYC - 1)
    def dispatch(kz, peer):
        place = steps.index((n_z - kz) % n_z) * NYC + yc
        remote(going.at[peer[0]], came.at[place], OUT, peer).start()

    to_all(dispatch)
    came[(n_z - 1) * NYC + yc] = going[me]

    wait_in(dw.at[pl.ds(0, NYC // 2 - 1)], DW)
    sibling = (z * NYC + yc + 1 - 2 * lax.rem(yc, 2), t)
    for k in range(0, NYC, 2):
        held = lax.rem(yc + k, NYC)
        remote(dw.at[held], dw.at[held], DW2, sibling).start()
    wait_in(dw.at[pl.ds(0, NYC // 2)], DW2)
    wait_in(dx.at[pl.ds(0, n_z - 1)], DX)
    dense_rows = dx[...].reshape(n_z * seqs, width)
    for i in range(2):
        weights = dw[:, i * UNITS : (i + 1) * UNITS].reshape(NYC * UNITS, width)
        dz_going[:, :, i * NYC * UNITS : (i + 1) * NYC * UNITS] = (
            dot_rows(dense_rows, weights).astype(BF16).reshape(n_tp, -1, NYC * UNITS)
        )
    for k in range(1, n_tp):
        peer = across_tp(k)
        remote(dz_going.at[peer[1]], dz_came.at[t], DZ, peer).start()
    dz_came[t] = dz_going[t]

    wait_in(came.at[pl.ds(0, n_ep - 1)], OUT)
    tall[...] = came[...].astype(F32).reshape(tall.shape)
    for j in range(lines):
        xs[:, j * 128 : (j + 1) * 128] = tall[pl.ds(j, slots, stride=lines), :].astype(BF16)
    loads[0].wait()
    loads[1].wait()
    rows = xs[...]
    act[...] = (jax.nn.silu(dot_rows(rows, w_gate[...])) * dot_rows(rows, w_up[...])).astype(BF16)
    loads[2].wait()
    halves = [pl.ds(0, n_ep), pl.ds(n_ep, n_ep)]
    for k in range(1, n_tp):
        peer = across_tp(k)
        columns = pl.ds(pl.multiple_of(peer[1] * width, width), width)
        moe_going[peer[1]] = dot(act[...], w_down[:, columns]).astype(BF16)
        half = (peer[1], halves[0])
        remote(moe_going.at[half], moe_came.at[t, halves[0]], MOE, peer).start()
    for k in range(1, n_tp):
        peer = across_tp(k)
        half = (peer[1], halves[1])
        remote(moe_going.at[half], moe_came.at[t, halves[1]], MOE2, peer).start()
    moe_came[t] = dot(act[...], w_down[:, own]).astype(BF16)

    wait_in(dz_came.at[pl.ds(0, n_tp - 1)], DZ)
    gate_up = dz_came[0].astype(F32)
    for k in range(1, n_tp):
        gate_up = gate_up + dz_came[k].astype(F32)
    hid[t] = (
        jax.nn.silu(gate_up[:, : NYC * UNITS]) * gate_up[:, NYC * UNITS :]
    ).astype(BF16)
    for k in range(1, n_tp):
        remote(hid.at[t], hid.at[t], HID, across_tp(k)).start()

    for n, which in enumerate((MOE, MOE2)):
        wait_in(moe_came.at[pl.ds(0, n_tp - 1), halves[n]], which)
        rows_out = moe_came[0, halves[n]].astype(F32)
        for k in range(1, n_tp):
            rows_out = rows_out + moe_came[k, halves[n]].astype(F32)
        lines = pl.ds(n * slots, slots)
        for j in range(width // 128):
            tall_back[pl.ds(n * slots + j, n_ep, stride=2), :] = rows_out[:, j * 128 : (j + 1) * 128]
        back_going[pl.ds(n * n_ep // 2, n_ep // 2)] = (
            tall_back[lines].reshape(n_ep // 2, 4, 128).astype(BF16)
        )

        def give_back(kz, peer):
            place = steps.index(kz) * NYC + peer[0] % NYC
            remote(back_going.at[place], back_came.at[me], BACK, peer).start()

        to_all(give_back, steps[n * n_z // 2 : (n + 1) * n_z // 2])
    back_came[me] = back_going[(n_z - 1) * NYC + yc]

    wait_in(hid.at[pl.ds(0, n_tp - 1)], HID)
    dense_part = dot(
        hid[...].reshape(n_z * seqs, NYC * UNITS),
        dw[:, 2 * UNITS : 3 * UNITS].reshape(NYC * UNITS, width),
    )
    od_going[...] = dense_part.astype(BF16).reshape(od_going.shape)

    for k in steps[:-1]:
        there = lax.rem(z + k, n_z)
        remote(od_going.at[there], od_came.at[z], OD, along_z(k)).start()
    od_came[z] = od_going[z]

    wait_in(od_came.at[pl.ds(0, n_z - 1)], OD)
    dense_out = od_came[0].astype(F32)
    for k in range(1, n_z):
        dense_out = dense_out + od_came[k].astype(F32)

    wait_in(back_came.at[pl.ds(0, n_ep - 1)], BACK)
    tall_back[...] = back_came[...].astype(F32).reshape(tall_back.shape)
    returned = [
        tall_back[pl.ds(j, slots, stride=2), :].astype(BF16) for j in range(width // 128)
    ]
    returned = jnp.concatenate(returned, axis=1).astype(F32)
    expert_out = jnp.dot(combine_ref[...], returned, precision=lax.Precision.HIGHEST)
    out_ref[...] = (
        residual_ref[:, own] + expert_out + dense_scale_ref[...] * dense_out
    ).astype(BF16)

    wait_out(parts.at[pl.ds(0, n_tp - 1)], PART)
    wait_out(dw.at[pl.ds(0, NYC // 2 - 1)], DW)
    wait_out(dw.at[pl.ds(0, NYC // 2)], DW2)
    wait_out(dx.at[pl.ds(0, n_z - 1)], DX)
    wait_out(going.at[pl.ds(0, n_ep - 1)], OUT)
    wait_out(dz_going.at[pl.ds(0, n_tp - 1)], DZ)
    wait_out(hid.at[pl.ds(0, n_tp - 1)], HID)
    wait_out(moe_going.at[pl.ds(0, n_tp - 1), halves[0]], MOE)
    wait_out(moe_going.at[pl.ds(0, n_tp - 1), halves[1]], MOE2)
    wait_out(back_going.at[pl.ds(0, n_ep - 1)], BACK)
    wait_out(od_going.at[pl.ds(0, n_z - 1)], OD)


def write_kernel(*refs):
    sems = refs[-1]
    copies = [pltpu.make_async_copy(refs[i], refs[4 + i], sems.at[i]) for i in (3, 0, 1, 2)]
    for copy in copies:
        copy.start()
    for copy in copies:
        copy.wait()


VMEM = pl.BlockSpec(memory_space=pltpu.VMEM)
ANY = pl.BlockSpec(memory_space=pl.ANY)


def local(
    n_ep,
    n_tp,
    tokens,
    mixer_gain,
    gate_weight,
    inner_weight,
    state_weight,
    step_weight,
    step_bias,
    decay_log,
    skip_scale,
    inner_kernel,
    state_kernel,
    inner_window,
    state_window,
    recurrent_state,
    group_gain,
    output_weight,
    channel_gain,
    routes,
    route_weights,
    expert_gate,
    expert_up,
    expert_down,
    dense_gate,
    dense_up,
    dense_down,
    dense_scale,
):
    seqs, model = tokens.shape
    width = dense_scale.shape[0]
    hidden = expert_gate.shape[2]
    n_z = n_ep // NYC
    slots = 2 * n_ep
    early = (
        tokens,
        mixer_gain[None],
        step_weight.T,
        step_bias[None],
        decay_log[None],
        skip_scale[None],
        inner_kernel,
        state_kernel,
        jnp.swapaxes(inner_window, 0, 1),
        state_window,
        group_gain[None],
    )
    late = (
        channel_gain[None],
        routes.T,
        route_weights.T,
        dense_gate.T,
        dense_up.T,
        dense_down,
        dense_scale[None],
    )
    scratch = [
        pltpu.VMEM(gate_weight.shape, BF16),
        pltpu.VMEM(inner_weight.shape, BF16),
        pltpu.VMEM(state_weight.shape, BF16),
        pltpu.VMEM(output_weight.shape, BF16),
        pltpu.VMEM((seqs, step_bias.shape[0] * STATE_DIM), F32),
        pltpu.VMEM((hidden, model), BF16),
        pltpu.VMEM((hidden, model), BF16),
        pltpu.VMEM((hidden, model), BF16),
        pltpu.VMEM((n_tp, seqs, model), BF16),
        pltpu.VMEM((seqs, model), F32),
        pltpu.VMEM((seqs, model), BF16),
        pltpu.VMEM((NYC, 3 * UNITS, width), BF16),
        pltpu.VMEM((n_z, seqs, width), BF16),
        pltpu.VMEM((seqs, slots), F32),
        pltpu.VMEM((slots * model // 128, 128), F32),
        pltpu.VMEM((n_ep, 2 * model // 128, 128), BF16),
        pltpu.VMEM((n_ep, 2 * model // 128, 128), BF16),
        pltpu.VMEM((slots, model), BF16),
        pltpu.VMEM((slots, hidden), BF16),
        pltpu.VMEM((n_tp, n_z * seqs // n_tp, 2 * NYC * UNITS), BF16),
        pltpu.VMEM((n_tp, n_z * seqs // n_tp, 2 * NYC * UNITS), BF16),
        pltpu.VMEM((n_tp, n_z * seqs // n_tp, NYC * UNITS), BF16),
        pltpu.VMEM((n_tp, slots, width), BF16),
        pltpu.VMEM((n_tp, slots, width), BF16),
        pltpu.VMEM((slots * 2, 128), F32),
        pltpu.VMEM((n_ep, 4, 128), BF16),
        pltpu.VMEM((n_ep, 4, 128), BF16),
        pltpu.VMEM((n_z, seqs, width), BF16),
        pltpu.VMEM((n_z, seqs, width), BF16),
        *[pltpu.VMEM(x.shape, x.dtype) for x in early],
        pltpu.SemaphoreType.DMA((len(early),)),
        *[pltpu.VMEM(x.shape, x.dtype) for x in late],
        pltpu.SemaphoreType.DMA((len(late),)),
        pltpu.SemaphoreType.DMA((4,)),
        pltpu.SemaphoreType.DMA((4,)),
        pltpu.SemaphoreType.DMA((3,)),
        pltpu.SemaphoreType.DMA((11,)),
        pltpu.SemaphoreType.DMA((11,)),
        pltpu.SemaphoreType.REGULAR((3,)),
    ]
    results = [
        ((seqs, width), BF16),
        ((3, seqs, width), BF16),
        (state_window.shape, BF16),
        (recurrent_state.shape, F32),
    ]
    held = pl.pallas_call(
        functools.partial(layer_kernel, n_ep, n_tp),
        out_shape=tuple(pltpu.VMEM(*r) for r in results),
        in_specs=[ANY] * 26,
        out_specs=(VMEM,) * 4,
        scratch_shapes=scratch,
        compiler_params=pltpu.CompilerParams(collective_id=0, has_side_effects=True),
        name="layer",
    )(
        *early,
        *late,
        gate_weight,
        inner_weight,
        state_weight,
        output_weight,
        recurrent_state,
        jnp.swapaxes(expert_gate, 1, 2),
        jnp.swapaxes(expert_up, 1, 2),
        expert_down,
    )
    new_tokens, new_inner, new_window, new_state = pl.pallas_call(
        write_kernel,
        out_shape=tuple(jax.ShapeDtypeStruct(*r) for r in results),
        in_specs=[VMEM] * 4,
        out_specs=(ANY,) * 4,
        scratch_shapes=[pltpu.SemaphoreType.DMA((4,))],
        name="write",
    )(*(pltpu.with_memory_space_constraint(h, pltpu.VMEM) for h in held))
    return new_tokens, new_state, jnp.swapaxes(new_inner, 0, 1), new_window


def solution(mesh):
    placed = (
        P("ep", None),
        P(),
        P(None, "tp"),
        P(None, "tp"),
        P(None, None, "tp"),
        P(None, "tp"),
        P("tp"),
        P("tp"),
        P("tp"),
        P(None, "tp"),
        P(None, None, "tp"),
        P("ep", None, "tp"),
        P("ep", None, None, "tp"),
        P("ep", "tp", None, None),
        P("tp"),
        P("tp", None),
        P(),
        P("ep", None),
        P("ep", None),
        P("ep", None, "tp"),
        P("ep", None, "tp"),
        P("ep", "tp", None),
        P("tp", "ep"),
        P("tp", "ep"),
        P("ep", "tp"),
        P("tp"),
    )
    return jax.shard_map(
        functools.partial(local, mesh.shape["ep"], mesh.shape["tp"]),
        mesh=mesh,
        in_specs=placed,
        out_specs=(
            P("ep", "tp"),
            P("ep", "tp", None, None),
            P("ep", None, "tp"),
            P("ep", None, None, "tp"),
        ),
        check_vma=False,
    )
```
